256 devices in a mesh: grp: 2 (over y), sp: 16 (over z), tp: 8 (over x, core).
Axes of the slice: x: 4, y: 2, z: 16, core: 2. Of those that a mesh axis runs over, the one named last changes fastest.
The devices are a block of a 4x16x16 slice.
Arguments:
- latent: bfloat16 [49152, 2048], P(('grp', 'sp')), parts along dimension 0, may hold values from -6 to 6
- condition: bfloat16 [4096], P('grp'), parts along dimension 0, may hold values from -6 to 6
- context_tokens: bfloat16 [512, 2048], P(('grp', 'sp')), parts along dimension 0, may hold values from -6 to 6
- context_condition: bfloat16 [2048], replicated, may hold values from -6 to 6
- shift_weight: bfloat16 [2048, 2048], P('sp', 'tp'), may hold values from -0.25 to 0.25
- scale_weight: bfloat16 [2048, 2048], P('sp', 'tp'), may hold values from -0.25 to 0.25
- gate_weight: bfloat16 [2048, 2048], P('sp', 'tp'), may hold values from -0.25 to 0.25
- norm_gain: bfloat16 [2048], replicated, may hold values from 0.099609375 to 1.8984375
- query_weight: bfloat16 [2048, 1024], P(None, 'tp'), may hold values from -0.125 to 0.125
- key_weight: bfloat16 [2048, 1024], P(None, 'tp'), may hold values from -0.125 to 0.125
- value_weight: bfloat16 [2048, 1024], P(None, 'tp'), may hold values from -0.125 to 0.125
- out_weight: bfloat16 [1024, 2048], replicated, may hold values from -0.1875 to 0.1875
- offset_bias: float32 [16, 15, 31], P('tp'), may hold values from 0.5 to 260
Outputs:
- mixed_latent: bfloat16 [49152, 2048], P(('grp', 'sp', 'tp')), parts along dimension 0
The draws below stay inside these ranges and needn't reach their ends.
There are 2 independent parts, one for each index of `grp`. The reference program is written for one: setup_inputs(seed, part) draws one part's arguments, and reference() takes and returns one part's arrays. A program takes and returns all parts, laid end to end along the dimension named above; an argument that names none is the same for every part. Nothing has to cross between parts.
All inputs are finite; a program needn't handle non-finite values.
Results may differ from the reference program's by a relative error of at most 0.011.
Values may be sent and summed in bfloat16 or wider, within the bound.
A program may use at most 128 MiB of HBM per device.

```python
import jax
import jax.numpy as jnp
import numpy as np
from jax import lax

D = 2048
HEADS = 16
HEAD_DIM = 64
ATT = 1024
GRID_W = 64
WIN_ROWS = 8
WIN_COLS = 16
COL_BLOCK = 16
CTX = 256
TOKENS = 24576


def draw_offset_bias(key, part):
    keys_all = jax.random.split(key, 1)
    table_shape = (HEADS, 2 * WIN_ROWS - 1, 2 * WIN_COLS - 1)
    bias_table = jax.random.uniform(keys_all[0], table_shape, jnp.float32, 0.5, 2.5)
    return bias_table


def shard_levels(key, dims, cuts, least, top_value):
    level, own = 1.0, jax.random.fold_in(key, 6)
    for dim, blocks in cuts:
        steps = jnp.exp(jax.random.uniform(jax.random.fold_in(own, dim), (blocks,), jnp.float32, least / len(cuts), top_value / len(cuts)))
        level = level * jnp.repeat(steps, dims[dim] // blocks).reshape([-1 if axis == dim else 1 for axis in range(len(dims))])
    return level


def centred(stream_key, shape, width, limit, cuts=(), kind=jnp.bfloat16):
    loudness = shard_levels(stream_key, shape, cuts, -0.22, 0.18) if cuts else 1.0
    array = jax.random.normal(stream_key, shape, jnp.float32) * width * loudness
    return jnp.minimum(jnp.maximum(array, -limit), limit).astype(kind)


def setup_inputs(seed: int = 0, part: int = 0) -> dict:
    key_of = jax.random.split(jax.random.key(seed), 14)
    part_keys = jax.random.split(jax.random.fold_in(key_of[13], part), 14)
    return {
        "latent": centred(part_keys[0], (TOKENS, D), 1.0, 6.0, ((0, 16),)),
        "condition": centred(part_keys[1], (D,), 1.0, 6.0),
        "context_tokens": centred(part_keys[2], (CTX, D), 1.0, 6.0, ((0, 16),)),
        "context_condition": centred(key_of[3], (D,), 1.0, 6.0),
        "shift_weight": centred(key_of[4], (D, D), (D // 4) ** -0.5, 0.25, ((0, 16), (1, 8))),
        "scale_weight": centred(key_of[5], (D, D), (D // 4) ** -0.5, 0.25, ((0, 16), (1, 8))),
        "gate_weight": centred(key_of[6], (D, D), (D // 4) ** -0.5, 0.25, ((0, 16), (1, 8))),
        "norm_gain": jnp.clip(1.0 + 0.18 * jax.random.normal(key_of[7], (D,), jnp.float32), 0.099609375, 1.8984375).astype(jnp.bfloat16),
        "query_weight": centred(key_of[8], (D, ATT), D ** -0.5, 0.125, ((1, 8),)),
        "key_weight": centred(key_of[9], (D, ATT), D ** -0.5, 0.125, ((1, 8),)),
        "value_weight": centred(key_of[10], (D, ATT), D ** -0.5, 0.125, ((1, 8),)),
        "out_weight": centred(key_of[11], (ATT, D), ATT ** -0.5, 0.1875),
        "offset_bias": draw_offset_bias(jax.random.fold_in(key_of[13], 71), part),
    }


epsilon = 1e-06
masked_score = -1e+30

def column_tables():
    block_count = GRID_W // COL_BLOCK
    strip_width = COL_BLOCK + WIN_COLS
    query_column = np.arange(GRID_W).reshape(block_count, COL_BLOCK)
    strip_start = np.clip(np.arange(block_count) * COL_BLOCK - WIN_COLS // 2, 0, GRID_W - strip_width)
    key_column = strip_start[:, None] + np.arange(strip_width)
    window_start = np.clip(query_column - WIN_COLS // 2, 0, GRID_W - WIN_COLS)
    inside = (key_column[:, None, :] >= window_start[..., None]) & (key_column[:, None, :] < window_start[..., None] + WIN_COLS)
    column_offset = np.clip(key_column[:, None, :] - query_column[..., None] + WIN_COLS - 1, 0, 2 * WIN_COLS - 2)
    return (strip_start, inside, column_offset)

def modulate_rows(tokens, norm_gain, shift_vector, scale_vector):
    values = tokens.astype(jnp.float32)
    normed = values * lax.rsqrt(lax.optimization_barrier(jnp.mean(values * values, axis=-1, keepdims=True)) + epsilon)
    return (normed * norm_gain.astype(jnp.float32) * (1.0 + scale_vector) + shift_vector).astype(jnp.bfloat16)

def neighbour_attention(queries, key_rows, value_rows, context_keys, context_values, offset_bias):
    heads_total = offset_bias.shape[0]
    grid_rows = queries.shape[0] // GRID_W
    block_count = GRID_W // COL_BLOCK
    strip_width = COL_BLOCK + WIN_COLS
    strip_start, inside, column_offset = column_tables()
    query_grid = queries.astype(jnp.float32).reshape(grid_rows, block_count, COL_BLOCK, heads_total, HEAD_DIM)
    key_grid = key_rows.astype(jnp.float32).reshape(grid_rows, GRID_W, heads_total, HEAD_DIM)
    value_grid = value_rows.astype(jnp.float32).reshape(grid_rows, GRID_W, heads_total, HEAD_DIM)
    far_keys = context_keys.astype(jnp.float32).reshape(-1, heads_total, HEAD_DIM)
    far_values = context_values.astype(jnp.float32).reshape(-1, heads_total, HEAD_DIM)
    factor = HEAD_DIM ** (-0.5)
    bias_table = offset_bias.astype(jnp.float32)

    def one_row(grid_row):
        first_row = jnp.clip(grid_row - WIN_ROWS // 2, 0, grid_rows - WIN_ROWS)
        key_window = lax.dynamic_slice_in_dim(key_grid, first_row, WIN_ROWS, 0)
        value_window = lax.dynamic_slice_in_dim(value_grid, first_row, WIN_ROWS, 0)
        key_strip = jnp.stack([key_window[:, int(column_begin):int(column_begin) + strip_width] for column_begin in strip_start], axis=1)
        value_strip = jnp.stack([value_window[:, int(column_begin):int(column_begin) + strip_width] for column_begin in strip_start], axis=1)
        query_row = lax.dynamic_index_in_dim(query_grid, grid_row, 0, keepdims=False)
        row_offset = first_row + jnp.arange(WIN_ROWS, dtype=jnp.int32) - grid_row + WIN_ROWS - 1
        bias_rows = bias_table[:, row_offset]
        bias_full = bias_rows[:, :, column_offset]
        near_scores = jnp.einsum('nqhd,wnkhd->hnqwk', query_row, key_strip) * factor + jnp.transpose(bias_full, (0, 2, 3, 1, 4))
        near_scores = jnp.where(inside[None, :, :, None, :], near_scores, masked_score)
        far_scores = jnp.einsum('nqhd,chd->hnqc', query_row, far_keys) * factor
        score_peak = jnp.maximum(lax.optimization_barrier(jnp.max(near_scores, axis=(3, 4))), lax.optimization_barrier(jnp.max(far_scores, axis=3)))
        near_exp = jnp.exp(near_scores - score_peak[..., None, None])
        far_exp = jnp.exp(far_scores - score_peak[..., None])
        denominator = lax.optimization_barrier(jnp.sum(near_exp, axis=(3, 4))) + lax.optimization_barrier(jnp.sum(far_exp, axis=3))
        near_weights = (near_exp / denominator[..., None, None]).astype(jnp.bfloat16).astype(jnp.float32)
        far_weights = (far_exp / denominator[..., None]).astype(jnp.bfloat16).astype(jnp.float32)
        output = jnp.einsum('hnqwk,wnkhd->nqhd', near_weights, value_strip) + jnp.einsum('hnqc,chd->nqhd', far_weights, far_values)
        return output.astype(jnp.bfloat16).reshape(GRID_W, heads_total * HEAD_DIM)
    rows_out = lax.map(one_row, jnp.arange(grid_rows, dtype=jnp.int32))
    return rows_out.reshape(grid_rows * GRID_W, heads_total * HEAD_DIM)

def reference(latent, condition, context_tokens, context_condition, shift_weight, scale_weight, gate_weight, norm_gain, query_weight, key_weight, value_weight, out_weight, offset_bias):
    cond_act = jax.nn.silu(condition.astype(jnp.float32)).astype(jnp.bfloat16)
    context_act = jax.nn.silu(context_condition.astype(jnp.float32)).astype(jnp.bfloat16)
    shift_vector = jnp.dot(cond_act, shift_weight, preferred_element_type=jnp.float32)
    scale_vector = jnp.dot(cond_act, scale_weight, preferred_element_type=jnp.float32)
    gate_vector = jnp.dot(cond_act, gate_weight, preferred_element_type=jnp.float32)
    context_shift = jnp.dot(context_act, shift_weight, preferred_element_type=jnp.float32)
    context_scale = jnp.dot(context_act, scale_weight, preferred_element_type=jnp.float32)
    hidden = modulate_rows(latent, norm_gain, shift_vector, scale_vector)
    context_hidden = modulate_rows(context_tokens, norm_gain, context_shift, context_scale)
    queries = jnp.dot(hidden, query_weight, preferred_element_type=jnp.float32).astype(jnp.bfloat16)
    key_rows = jnp.dot(hidden, key_weight, preferred_element_type=jnp.float32).astype(jnp.bfloat16)
    value_rows = jnp.dot(hidden, value_weight, preferred_element_type=jnp.float32).astype(jnp.bfloat16)
    context_keys = jnp.dot(context_hidden, key_weight, preferred_element_type=jnp.float32).astype(jnp.bfloat16)
    context_values = jnp.dot(context_hidden, value_weight, preferred_element_type=jnp.float32).astype(jnp.bfloat16)
    attended = neighbour_attention(queries, key_rows, value_rows, context_keys, context_values, offset_bias)
    branch = jnp.dot(attended, out_weight, preferred_element_type=jnp.float32)
    return (latent.astype(jnp.float32) + gate_vector * branch).astype(jnp.bfloat16)
```

```python
import functools

import jax
import jax.numpy as jnp
from jax import lax
from jax.experimental import pallas as pl
from jax.experimental.pallas import tpu as pltpu
from jax.sharding import PartitionSpec as P

HEAD_DIM = 64
GRID_W = 64
WIN_ROWS = 8
WIN_COLS = 16
COL_BLOCK = 16
STRIP = COL_BLOCK + WIN_COLS
BLOCKS = GRID_W // COL_BLOCK
HALO = WIN_ROWS // 2
STARTS = (0, 8, 24, 32)
VARIANT = (0, 1, 1, 2)
SHIFTS = (15, 7, -1)
EPS = 1e-6
MASKED = -1e30
LANES = 128

bf16 = jnp.bfloat16
f32 = jnp.float32
MESH = pl.DeviceIdType.MESH


def dot(a, b):
    return jnp.dot(a, b, preferred_element_type=f32)


def dot_nt(a, b):
    return lax.dot_general(a, b, (((1,), (1,)), ((), ())), preferred_element_type=f32)


def kernel(
    n_sp,
    n_tp,
    latent,
    cond,
    ctx_tokens,
    ctx_cond,
    shift_w,
    scale_w,
    gate_w,
    gain,
    query_w,
    key_w,
    value_w,
    out_w,
    bias,
    out,
    X,
    CD,
    XD,
    CT,
    MW,
    GN,
    W,
    W2,
    WO,
    BI,
    PAD,
    TP,
    TB,
    RS,
    P1,
    R1,
    P2,
    R2,
    LH,
    CS,
    CR,
    CV,
    QS,
    KS,
    VS,
    HB,
    HR,
    AS,
    AR,
    OB,
    load_sem,
    p1_send,
    p1_recv,
    p2_send,
    p2_recv,
    c_send,
    c_recv,
    h_send,
    h_recv,
    a_send,
    a_recv,
    o_sem,
):
    sp = lax.axis_index("sp")
    tp = lax.axis_index("tp")
    tokens, width = X.shape
    ft = width // n_tp
    rows = tokens // GRID_W
    crows = rows // n_tp
    share = crows * GRID_W
    urows = crows + WIN_ROWS - 1
    ukeys = urows * STRIP
    qrows = crows * 2 * COL_BLOCK
    att = W.shape[1] // 3

    barrier = pltpu.get_barrier_semaphore()

    def greet_sp(k, c):
        pl.semaphore_signal(
            barrier, inc=1, device_id={"sp": lax.rem(sp + k, n_sp)}, device_id_type=MESH
        )
        return c

    def greet_tp(k, c):
        pl.semaphore_signal(
            barrier, inc=1, device_id={"tp": lax.rem(tp + k, n_tp)}, device_id_type=MESH
        )
        return c

    lax.fori_loop(1, n_sp, greet_sp, 0)
    lax.fori_loop(1, n_tp, greet_tp, 0)

    loads = [
        (cond, CD),
        (ctx_cond, XD),
        (shift_w, MW.at[0]),
        (scale_w, MW.at[1]),
        (gate_w, MW.at[2]),
        (bias, BI),
        (gain, GN),
        (ctx_tokens, CT),
        (latent, X),
        (query_w, W.at[:, pl.ds(0, att)]),
        (key_w, W.at[:, pl.ds(att, att)]),
        (value_w, W.at[:, pl.ds(2 * att, att)]),
        (out_w, WO),
    ]
    loads = [
        pltpu.make_async_copy(src, dst, load_sem.at[i]) for i, (src, dst) in enumerate(loads)
    ]
    for copy in loads:
        copy.start()

    row8 = lax.broadcasted_iota(jnp.int32, (8, ft), 0)

    for copy in loads[:5]:
        copy.wait()

    def own_act(ref):
        v = ref[...].astype(f32)
        act = (v / (1.0 + jnp.exp(-v))).astype(bf16).astype(f32)
        own = lax.broadcasted_iota(jnp.int32, act.shape, 0) == sp
        return jnp.sum(jnp.where(own, act, 0.0), axis=0, keepdims=True)

    own_cond, own_ctx = own_act(CD), own_act(XD)
    r16 = lax.broadcasted_iota(jnp.int32, (16, own_cond.shape[1]), 0)
    acts = jnp.where(r16 == 0, own_cond, jnp.where(r16 == 1, own_ctx, 0.0)).astype(bf16)
    d_shift, d_scale, d_gate = dot(acts, MW[0]), dot(acts, MW[1]), dot(acts, MW[2])
    terms = (d_shift[0:1], d_scale[0:1], d_gate[0:1], d_shift[1:2], d_scale[1:2])
    packed = jnp.zeros((8, ft), f32)
    for i, term in enumerate(terms):
        packed = jnp.where(row8 == i, term, packed)
    P1[...] = packed
    R1[sp] = packed

    pl.semaphore_wait(barrier, n_sp - 1 + n_tp - 1)

    def p1_copy(k):
        peer = lax.rem(sp + k, n_sp)
        return pltpu.make_async_remote_copy(
            src_ref=P1,
            dst_ref=R1.at[sp],
            send_sem=p1_send.at[peer],
            recv_sem=p1_recv.at[sp],
            device_id={"sp": peer},
            device_id_type=MESH,
        )

    def p1_arrival(k):
        peer = lax.rem(sp + k, n_sp)
        return pltpu.make_async_remote_copy(
            src_ref=P1,
            dst_ref=R1.at[peer],
            send_sem=p1_send.at[peer],
            recv_sem=p1_recv.at[peer],
            device_id={"sp": peer},
            device_id_type=MESH,
        )

    def p1_start(k, c):
        p1_copy(k).start()
        return c

    lax.fori_loop(1, n_sp, p1_start, 0)

    loads[5].wait()
    lane = lax.broadcasted_iota(jnp.int32, (COL_BLOCK, LANES), 1)
    in_group = lax.rem(lane, STRIP)
    query = lax.broadcasted_iota(jnp.int32, (COL_BLOCK, LANES), 0)
    lower = (
        jnp.maximum(query - WIN_COLS // 2, 0),
        query,
        jnp.minimum(query + WIN_COLS // 2, WIN_COLS),
    )
    inside = [(in_group >= lo) & (in_group < lo + WIN_COLS) for lo in lower]
    offsets = 2 * WIN_ROWS - 1
    PAD[...] = jnp.zeros_like(PAD)
    for h in range(2):
        PAD[h, pl.ds(0, offsets), pl.ds(0, 2 * WIN_COLS - 1)] = BI[h]
        x = PAD[h]
        x = x + pltpu.roll(x, 32, 1)
        PAD[h] = x + pltpu.roll(x, 64, 1)

    def lay_out(o, c):
        for h in range(2):
            line = jnp.broadcast_to(PAD[h, pl.ds(o, 1), :], (COL_BLOCK, LANES))
            for v in range(3):
                turned = pltpu.roll(line, (-SHIFTS[v]) % LANES, 1, stride=1, stride_axis=0)
                TP[v, h, o] = jnp.where(inside[v], turned, MASKED)
        return c

    lax.fori_loop(0, offsets, lay_out, 0)
    group = lane // STRIP
    per = LANES // STRIP
    variants = (
        (-HALO, lambda i: i),
        (0, lambda i: 0),
        (-crows, lambda i: max(crows + i - HALO, 0)),
        (-(urows - crows), lambda i: urows - WIN_ROWS),
    )

    def assemble(vh, c):
        v, h = vh // 2, lax.rem(vh, 2)
        for rv, (delta, first) in enumerate(variants):
            for i in range(crows):
                for g in range(TB.shape[-1] // LANES):
                    tile = jnp.full((COL_BLOCK, LANES), MASKED, f32)
                    for l in range(per):
                        j = g * per + l
                        if first(i) <= j < first(i) + WIN_ROWS and j < urows:
                            o = delta + j - i + WIN_ROWS - 1
                            tile = jnp.where(group == l, TP[v, h, o], tile)
                    TB[rv, v, i, h, :, pl.ds(g * LANES, LANES)] = tile
        return c

    lax.fori_loop(0, 6, assemble, 0)

    loads[8].wait()

    def norms(k, c):
        at = pl.ds(pl.multiple_of(k * 16, 16), 16)
        x = X[at, :].astype(f32)
        mean = jnp.sum(x * x, axis=1, keepdims=True) * (1.0 / width)
        RS[at, :] = jnp.broadcast_to(lax.rsqrt(mean + EPS), (16, LANES))
        return c

    lax.fori_loop(0, tokens // 16, norms, 0)
    loads[6].wait()
    loads[7].wait()
    for copy in loads[9:12]:
        copy.wait()

    CV[:, pl.ds(LANES, LANES)] = jnp.ones((CV.shape[0], LANES), bf16)

    def fill(r, c):
        for b in range(BLOCKS):
            VS[b, r, :, pl.ds(LANES, LANES)] = jnp.ones((STRIP, LANES), bf16)
        return c

    lax.fori_loop(0, rows + 2 * HALO, fill, 0)

    def p1_wait(k, c):
        p1_arrival(k).wait_recv()
        return c

    lax.fori_loop(1, n_sp, p1_wait, 0)
    summed = jnp.sum(R1[...], axis=0)
    P2[...] = summed
    R2[tp] = summed

    def p2_copy(k, slot):
        peer = lax.rem(tp + k, n_tp)
        return pltpu.make_async_remote_copy(
            src_ref=P2,
            dst_ref=R2.at[tp if slot is None else peer],
            send_sem=p2_send.at[peer],
            recv_sem=p2_recv.at[tp if slot is None else peer],
            device_id={"tp": peer},
            device_id_type=MESH,
        )

    def p2_start(k, c):
        p2_copy(k, None).start()
        return c

    lax.fori_loop(1, n_tp, p2_start, 0)

    def p2_wait(k, c):
        p2_copy(k, 1).wait_recv()
        return c

    lax.fori_loop(1, n_tp, p2_wait, 0)

    ctx_rows = CT.shape[0]
    sq = jnp.zeros((ctx_rows, 1), f32)
    for t in range(n_tp):
        x = CT[:, pl.ds(t * ft, ft)].astype(f32)
        sq = sq + jnp.sum(x * x, axis=1, keepdims=True)
    ctx_scale = lax.rsqrt(sq * (1.0 / width) + EPS)
    r16 = lax.broadcasted_iota(jnp.int32, (16, ft), 0)
    for t in range(n_tp):
        cols = pl.ds(t * ft, ft)
        x = CT[:, cols].astype(f32) * ctx_scale
        x = x * GN[pl.ds(t, 1), :].astype(f32) * (1.0 + R2[t, 4:5, :]) + R2[t, 3:4, :]
        LH[pl.ds(0, ctx_rows), cols] = x.astype(bf16)
        shift = R2[t, 0:1, :]
        high = shift.astype(bf16).astype(f32)
        low = shift - high
        pair = jnp.where(r16 == 0, high, jnp.where(r16 == 1, low, 0.0))
        LH[pl.ds(ctx_rows, 16), cols] = pair.astype(bf16)
    side = dot(LH[...], W[...])
    CS[...] = side[:ctx_rows, att:].astype(bf16)
    add = side[ctx_rows : ctx_rows + 1] + side[ctx_rows + 1 : ctx_rows + 2]

    def c_copy(k, slot):
        peer = lax.rem(sp + k, n_sp)
        return pltpu.make_async_remote_copy(
            src_ref=CS,
            dst_ref=CR.at[sp if slot is None else peer],
            send_sem=c_send.at[peer],
            recv_sem=c_recv.at[sp if slot is None else peer],
            device_id={"sp": peer},
            device_id_type=MESH,
        )

    def c_start(k, c):
        c_copy(k, None).start()
        return c

    lax.fori_loop(1, n_sp, c_start, 0)
    CR[sp] = CS[...]

    halves = ft // LANES
    scale = jnp.concatenate([R2[t, 1:2, :] for t in range(n_tp)], axis=0)
    factor = GN[...].astype(f32) * (1.0 + scale)
    slabs = [factor[:, s * LANES : (s + 1) * LANES] for s in range(halves)]
    slabs.append(jnp.zeros((LANES - halves * n_tp, LANES), f32))
    turned = jnp.concatenate(slabs, axis=0).T
    for s in range(halves):
        for t in range(n_tp):
            at = pl.ds(t * ft + s * LANES, LANES)
            column = turned[:, s * n_tp + t : s * n_tp + t + 1]
            W2[at, :] = (W[at, :].astype(f32) * column).astype(bf16)

    per_block = HALO * GRID_W
    steps = rows // HALO
    head0 = lax.broadcasted_iota(jnp.int32, (COL_BLOCK, LANES), 1) < HEAD_DIM

    def h_copy(side_):
        return pltpu.make_async_remote_copy(
            src_ref=HB.at[side_],
            dst_ref=HR.at[side_],
            send_sem=h_send.at[side_],
            recv_sem=h_recv.at[side_],
            device_id={"sp": lax.rem(sp + (1 if side_ == 0 else n_sp - 1), n_sp)},
            device_id_type=MESH,
        )

    def project(k, c):
        m = jnp.where(k == 0, 0, jnp.where(k == 1, steps - 1, k - 1))
        at = pl.ds(pl.multiple_of(m * per_block, per_block), per_block)
        acc = dot(X[at, :], W2[...])
        rs = RS[at, :]
        parts = [
            acc[:, p * att : (p + 1) * att] * rs + add[:, p * att : (p + 1) * att]
            for p in range(3)
        ]
        q = parts[0] * (HEAD_DIM**-0.5)
        for r in range(HALO):
            for b in range(BLOCKS):
                begin = r * GRID_W + b * COL_BLOCK
                piece = q[begin : begin + COL_BLOCK]
                QS[b, m * HALO + r, 0] = jnp.where(head0, piece, 0.0).astype(bf16)
                QS[b, m * HALO + r, 1] = jnp.where(head0, 0.0, piece).astype(bf16)
                begin = r * GRID_W + STARTS[b]
                KS[b, m * HALO + r + HALO] = parts[1][begin : begin + STRIP].astype(bf16)
                VS[b, m * HALO + r + HALO, :, pl.ds(0, LANES)] = parts[2][
                    begin : begin + STRIP
                ].astype(bf16)

        @pl.when(k < 2)
        def _():
            HB[1 - k, :, pl.ds(0, att)] = parts[1].astype(bf16)
            HB[1 - k, :, pl.ds(att, att)] = parts[2].astype(bf16)

        return c

    lax.fori_loop(0, 2, project, 0)

    @pl.when(sp < n_sp - 1)
    def _():
        h_copy(0).start()

    @pl.when(sp > 0)
    def _():
        h_copy(1).start()

    lax.fori_loop(2, steps, project, 0)

    def c_wait(k, c):
        c_copy(k, 1).wait_recv()
        return c

    lax.fori_loop(1, n_sp, c_wait, 0)
    for s in range(n_sp):
        CV[pl.ds(s * ctx_rows, ctx_rows), pl.ds(0, att)] = CR[s, :, pl.ds(att, att)]

    loads[12].wait()

    def spread(side_):
        first = 0 if side_ == 0 else rows + HALO
        for r in range(HALO):
            pair = HR[side_, pl.ds(r * GRID_W, GRID_W), :].astype(f32)
            for b in range(BLOCKS):
                strip = pair[STARTS[b] : STARTS[b] + STRIP].astype(bf16)
                KS[b, first + r] = strip[:, :att]
                VS[b, first + r, :, pl.ds(0, LANES)] = strip[:, att:]

    def a_copy(c, slot):
        return pltpu.make_async_remote_copy(
            src_ref=AS.at[c],
            dst_ref=AR.at[tp if slot is None else c],
            send_sem=a_send.at[c],
            recv_sem=a_recv.at[tp if slot is None else c],
            device_id={"tp": c},
            device_id_type=MESH,
        )

    low = -(-HALO // crows)
    inner = n_tp - 2 * low
    outer = 2 * low

    def attend(k, carry):
        @pl.when(k == inner)
        def _():
            @pl.when(sp > 0)
            def _():
                h_copy(0).wait_recv()
                spread(0)

            @pl.when(sp < n_sp - 1)
            def _():
                h_copy(1).wait_recv()
                spread(1)

        e = lax.rem(tp + 1 + k, outer)
        c = jnp.where(
            k < inner, low + lax.rem(tp + k, inner), jnp.where(e < low, e, e + inner)
        )
        rv = jnp.where(
            (sp == 0) & (c < 2), c + 1, jnp.where((sp == n_sp - 1) & (c == n_tp - 1), 3, 0)
        )
        base = jnp.where(
            (rv == 1) | (rv == 2), HALO, jnp.where(rv == 3, rows + HALO - urows, c * crows)
        )
        for b in range(BLOCKS):
            q2 = QS[b, pl.ds(c * crows, crows)].reshape(qrows, LANES)
            ks = KS[b, pl.ds(base, urows)].reshape(ukeys, LANES)
            near = dot_nt(q2, ks)
            table = TB[rv, VARIANT[b], :, :, :, pl.ds(0, ukeys)].reshape(qrows, ukeys)
            near = near + table
            far = dot_nt(q2, CR[:, :, pl.ds(0, att)].reshape(n_sp * ctx_rows, att))
            peak = jnp.maximum(
                jnp.max(near, axis=1, keepdims=True), jnp.max(far, axis=1, keepdims=True)
            )
            near = jnp.exp(near - peak).astype(bf16)
            far = jnp.exp(far - peak).astype(bf16)
            vs = VS[b, pl.ds(base, urows)].reshape(ukeys, 2 * LANES)
            both = dot(near, vs) + dot(far, CV[...])
            value = (both[:, :LANES] / both[:, LANES:]).reshape(crows, 2, COL_BLOCK, LANES)
            for i in range(crows):
                AS[c, pl.ds(i * GRID_W + b * COL_BLOCK, COL_BLOCK), :] = jnp.where(
                    head0, value[i, 0], value[i, 1]
                ).astype(bf16)

        @pl.when(c != tp)
        def _():
            a_copy(c, None).start()

        return carry

    lax.fori_loop(0, n_tp, attend, 0)

    AR[tp] = AS[tp]

    def a_wait(k, c):
        a_copy(lax.rem(tp + k, n_tp), 1).wait_recv()
        return c

    lax.fori_loop(1, n_tp, a_wait, 0)
    merged = jnp.concatenate([AR[t] for t in range(n_tp)], axis=1)
    own = pl.ds(pl.multiple_of(tp * share, share), share)
    stores = []
    for t in range(n_tp):
        cols = pl.ds(t * ft, ft)
        branch = dot(merged, WO[:, cols])
        OB[:, cols] = (X[own, cols].astype(f32) + R2[t, 2:3, :] * branch).astype(bf16)
        store = pltpu.make_async_copy(OB.at[:, cols], out.at[:, cols], o_sem.at[t])
        store.start()
        stores.append(store)

    def p1_done(k, c):
        p1_copy(k).wait_send()
        c_copy(k, None).wait_send()
        return c

    lax.fori_loop(1, n_sp, p1_done, 0)

    def p2_done(k, c):
        p2_copy(k, None).wait_send()
        a_copy(lax.rem(tp + k, n_tp), None).wait_send()
        return c

    lax.fori_loop(1, n_tp, p2_done, 0)

    @pl.when(sp < n_sp - 1)
    def _():
        h_copy(0).wait_send()

    @pl.when(sp > 0)
    def _():
        h_copy(1).wait_send()

    for store in stores:
        store.wait()


def local(n_sp, n_tp, *args):
    (
        latent,
        condition,
        context_tokens,
        context_condition,
        shift_weight,
        scale_weight,
        gate_weight,
        norm_gain,
        query_weight,
        key_weight,
        value_weight,
        out_weight,
        offset_bias,
    ) = args
    tokens, width = latent.shape
    inputs, ft = shift_weight.shape
    att = query_weight.shape[1]
    rows = tokens // GRID_W
    crows = rows // n_tp
    share = crows * GRID_W
    urows = crows + WIN_ROWS - 1
    ctx_rows = context_tokens.shape[0]
    table = -(-urows * STRIP // LANES) * LANES
    padded = rows + 2 * HALO
    operands = (
        latent,
        condition.reshape(n_sp, inputs),
        context_tokens,
        context_condition.reshape(n_sp, inputs),
        shift_weight,
        scale_weight,
        gate_weight,
        norm_gain.reshape(n_tp, ft),
        query_weight,
        key_weight,
        value_weight,
        out_weight,
        offset_bias,
    )
    dma = pltpu.SemaphoreType.DMA
    scratch = [
        pltpu.VMEM((tokens, width), bf16),
        pltpu.VMEM((n_sp, inputs), bf16),
        pltpu.VMEM((n_sp, inputs), bf16),
        pltpu.VMEM((ctx_rows, width), bf16),
        pltpu.VMEM((3, inputs, ft), bf16),
        pltpu.VMEM((n_tp, ft), bf16),
        pltpu.VMEM((width, 3 * att), bf16),
        pltpu.VMEM((width, 3 * att), bf16),
        pltpu.VMEM(out_weight.shape, bf16),
        pltpu.VMEM(offset_bias.shape, f32),
        pltpu.VMEM((2, 16, LANES), f32),
        pltpu.VMEM((3, 2, 2 * WIN_ROWS, COL_BLOCK, LANES), f32),
        pltpu.VMEM((4, 3, crows, 2, COL_BLOCK, table), f32),
        pltpu.VMEM((tokens, LANES), f32),
        pltpu.VMEM((8, ft), f32),
        pltpu.VMEM((n_sp, 8, ft), f32),
        pltpu.VMEM((8, ft), f32),
        pltpu.VMEM((n_tp, 8, ft), f32),
        pltpu.VMEM((ctx_rows + 16, width), bf16),
        pltpu.VMEM((ctx_rows, 2 * att), bf16),
        pltpu.VMEM((n_sp, ctx_rows, 2 * att), bf16),
        pltpu.VMEM((n_sp * ctx_rows, 2 * LANES), bf16),
        pltpu.VMEM((BLOCKS, rows, 2, COL_BLOCK, LANES), bf16),
        pltpu.VMEM((BLOCKS, padded, STRIP, LANES), bf16),
        pltpu.VMEM((BLOCKS, padded, STRIP, 2 * LANES), bf16),
        pltpu.VMEM((2, HALO * GRID_W, 2 * att), bf16),
        pltpu.VMEM((2, HALO * GRID_W, 2 * att), bf16),
        pltpu.VMEM((n_tp, share, LANES), bf16),
        pltpu.VMEM((n_tp, share, LANES), bf16),
        pltpu.VMEM((share, width), bf16),
        dma((13,)),
        dma((n_sp,)),
        dma((n_sp,)),
        dma((n_tp,)),
        dma((n_tp,)),
        dma((n_sp,)),
        dma((n_sp,)),
        dma((2,)),
        dma((2,)),
        dma((n_tp,)),
        dma((n_tp,)),
        dma((n_tp,)),
    ]
    return pl.pallas_call(
        functools.partial(kernel, n_sp, n_tp),
        out_shape=jax.ShapeDtypeStruct((share, width), bf16),
        in_specs=[pl.BlockSpec(memory_space=pl.ANY)] * len(operands),
        out_specs=pl.BlockSpec(memory_space=pl.ANY),
        scratch_shapes=scratch,
        compiler_params=pltpu.CompilerParams(
            collective_id=0, has_side_effects=True, vmem_limit_bytes=60 * 1024 * 1024
        ),
    )(*operands)


def solution(mesh):
    placed = (
        P(("grp", "sp"), None),
        P("grp"),
        P(("grp", "sp"), None),
        P(),
        P("sp", "tp"),
        P("sp", "tp"),
        P("sp", "tp"),
        P(),
        P(None, "tp"),
        P(None, "tp"),
        P(None, "tp"),
        P(),
        P("tp", None, None),
    )
    return jax.shard_map(
        functools.partial(local, mesh.shape["sp"], mesh.shape["tp"]),
        mesh=mesh,
        in_specs=placed,
        out_specs=P(("grp", "sp", "tp"), None),
        check_vma=False,
    )
```

```python
import functools

import jax
import jax.numpy as jnp
from jax import lax
from jax.experimental import pallas as pl
from jax.experimental.pallas import tpu as pltpu
from jax.sharding import PartitionSpec as P

HEAD_DIM = 64
GRID_W = 64
WIN_ROWS = 8
WIN_COLS = 16
COL_BLOCK = 16
STRIP = COL_BLOCK + WIN_COLS
BLOCKS = GRID_W // COL_BLOCK
HALO = WIN_ROWS // 2
STARTS = (0, 8, 24, 32)
VARIANT = (0, 1, 1, 2)
SHIFTS = (15, 7, -1)
EPS = 1e-6
MASKED = -1e30
LANES = 128

bf16 = jnp.bfloat16
f32 = jnp.float32
MESH = pl.DeviceIdType.MESH


def dot(a, b):
    return jnp.dot(a, b, preferred_element_type=f32)


def dot_nt(a, b):
    return lax.dot_general(a, b, (((1,), (1,)), ((), ())), preferred_element_type=f32)


def kernel(
    n_sp,
    n_tp,
    latent,
    cond,
    ctx_tokens,
    ctx_cond,
    shift_w,
    scale_w,
    gate_w,
    gain,
    query_w,
    key_w,
    value_w,
    out_w,
    bias,
    out,
    X,
    CD,
    XD,
    MW,
    GN,
    W,
    W2,
    WO,
    BI,
    PAD,
    TP,
    TB,
    RS,
    P1,
    R1,
    P2,
    R2,
    LH,
    W3,
    CX,
    CK,
    CV,
    QS,
    KS,
    VS,
    HB,
    HR,
    AS,
    AR,
    OB,
    load_sem,
    p1_send,
    p1_recv,
    p2_send,
    p2_recv,
    c_send,
    c_recv,
    x_send,
    x_recv,
    d_send,
    d_recv,
    t_send,
    t_recv,
    ready,
    h_send,
    h_recv,
    a_send,
    a_recv,
    o_sem,
):
    sp = lax.axis_index("sp")
    tp = lax.axis_index("tp")
    tokens, width = X.shape
    ft = width // n_tp
    rows = tokens // GRID_W
    crows = rows // n_tp
    share = crows * GRID_W
    urows = crows + WIN_ROWS - 1
    ukeys = urows * STRIP
    qrows = crows * 2 * COL_BLOCK
    att = W.shape[1] // 3

    barrier = pltpu.get_barrier_semaphore()

    def greet_sp(j, c):
        pl.semaphore_signal(barrier, inc=1, device_id={"sp": j}, device_id_type=MESH)
        return c

    def greet_tp(k, c):
        pl.semaphore_signal(
            barrier, inc=1, device_id={"tp": lax.rem(tp + k, n_tp)}, device_id_type=MESH
        )
        return c

    lax.fori_loop(sp + 1, n_sp, greet_sp, 0)
    lax.fori_loop(1, n_tp, greet_tp, 0)

    mine = pl.ds(pl.multiple_of(tp * ft, ft), ft)
    loads = [
        (shift_w, MW.at[0]),
        (scale_w, MW.at[1]),
        (gate_w, MW.at[2]),
        (cond, CD),
        (ctx_cond, XD),
        (ctx_tokens.at[:, mine], CX.at[sp, :, mine]),
        (bias, BI),
        (gain, GN),
        (latent, X),
        (query_w, W.at[:, pl.ds(0, att)]),
        (key_w, W.at[:, pl.ds(att, att)]),
        (value_w, W.at[:, pl.ds(2 * att, att)]),
        (out_w, WO),
    ]
    loads = [
        pltpu.make_async_copy(src, dst, load_sem.at[i]) for i, (src, dst) in enumerate(loads)
    ]
    for copy in loads:
        copy.start()

    row8 = lax.broadcasted_iota(jnp.int32, (8, ft), 0)

    for copy in loads[:5]:
        copy.wait()

    def own_act(ref):
        v = ref[...].astype(f32)
        act = (v / (1.0 + jnp.exp(-v))).astype(bf16).astype(f32)
        own = lax.broadcasted_iota(jnp.int32, act.shape, 0) == sp
        return jnp.sum(jnp.where(own, act, 0.0), axis=0, keepdims=True)

    own_cond, own_ctx = own_act(CD), own_act(XD)
    r16 = lax.broadcasted_iota(jnp.int32, (16, own_cond.shape[1]), 0)
    acts = jnp.where(r16 == 0, own_cond, jnp.where(r16 == 1, own_ctx, 0.0)).astype(bf16)
    d_shift, d_scale, d_gate = dot(acts, MW[0]), dot(acts, MW[1]), dot(acts, MW[2])
    terms = (d_shift[0:1], d_scale[0:1], d_gate[0:1], d_shift[1:2], d_scale[1:2])
    packed = jnp.zeros((8, ft), f32)
    for i, term in enumerate(terms):
        packed = jnp.where(row8 == i, term, packed)
    P1[...] = packed
    R1[sp] = packed

    def prepare():
        loads[6].wait()
        lane = lax.broadcasted_iota(jnp.int32, (COL_BLOCK, LANES), 1)
        in_group = lax.rem(lane, STRIP)
        query = lax.broadcasted_iota(jnp.int32, (COL_BLOCK, LANES), 0)
        lower = (
            jnp.maximum(query - WIN_COLS // 2, 0),
            query,
            jnp.minimum(query + WIN_COLS // 2, WIN_COLS),
        )
        inside = [(in_group >= lo) & (in_group < lo + WIN_COLS) for lo in lower]
        offsets = 2 * WIN_ROWS - 1
        PAD[...] = jnp.zeros_like(PAD)
        for h in range(2):
            PAD[h, pl.ds(0, offsets), pl.ds(0, 2 * WIN_COLS - 1)] = BI[:, h]
            x = PAD[h]
            x = x + pltpu.roll(x, 32, 1)
            PAD[h] = x + pltpu.roll(x, 64, 1)

        def lay_out(o, c):
            for h in range(2):
                line = jnp.broadcast_to(PAD[h, pl.ds(o, 1), :], (COL_BLOCK, LANES))
                for v in range(3):
                    turned = pltpu.roll(line, (-SHIFTS[v]) % LANES, 1, stride=1, stride_axis=0)
                    TP[v, h, o] = jnp.where(inside[v], turned, MASKED)
            return c

        lax.fori_loop(0, offsets, lay_out, 0)
        group = lane // STRIP
        per = LANES // STRIP
        variants = (
            (-HALO, lambda i: i),
            (0, lambda i: 0),
            (-crows, lambda i: max(crows + i - HALO, 0)),
            (-(urows - crows), lambda i: urows - WIN_ROWS),
        )

        def assemble(vh, c):
            v, h = vh // 2, lax.rem(vh, 2)
            for rv, (delta, first) in enumerate(variants):
                for i in range(crows):
                    for g in range(TB.shape[-1] // LANES):
                        tile = jnp.full((COL_BLOCK, LANES), MASKED, f32)
                        for l in range(per):
                            j = g * per + l
                            if first(i) <= j < first(i) + WIN_ROWS and j < urows:
                                o = delta + j - i + WIN_ROWS - 1
                                tile = jnp.where(group == l, TP[v, h, o], tile)
                        TB[rv, v, i, h, :, pl.ds(g * LANES, LANES)] = tile
            return c

        lax.fori_loop(0, 6, assemble, 0)

        loads[8].wait()

        def norms(k, c):
            for u in range(4):
                at = pl.ds(pl.multiple_of(k * 64 + u * 16, 16), 16)
                x = X[at, :].astype(f32)
                mean = jnp.sum(x * x, axis=1, keepdims=True) * (1.0 / width)
                RS[at, :] = jnp.broadcast_to(lax.rsqrt(mean + EPS), (16, LANES))
            return c

        lax.fori_loop(0, tokens // 64, norms, 0)
        loads[7].wait()
        for copy in loads[9:12]:
            copy.wait()

        CV[:, pl.ds(LANES, LANES)] = jnp.ones((CV.shape[0], LANES), bf16)

        def fill(r, c):
            for b in range(BLOCKS):
                VS[b, r, :, pl.ds(LANES, LANES)] = jnp.ones((STRIP, LANES), bf16)
            return c

        lax.fori_loop(0, rows + 2 * HALO, fill, 0)

    loads[5].wait()
    pl.semaphore_wait(barrier, sp + n_tp - 1)
    first_half = n_sp // 2
    partner = tp + 1 - 2 * lax.rem(tp, 2)

    def p1_copy(source):
        return pltpu.make_async_remote_copy(
            src_ref=P1,
            dst_ref=R1.at[source],
            send_sem=p1_send.at[0],
            recv_sem=p1_recv.at[source],
            device_id={"sp": 0},
            device_id_type=MESH,
        )

    def t_copy(peer):
        return pltpu.make_async_remote_copy(
            src_ref=P2,
            dst_ref=P2,
            send_sem=t_send.at[peer],
            recv_sem=t_recv.at[0],
            device_id={"sp": peer},
            device_id_type=MESH,
        )

    def c_copy(peer, slot):
        return pltpu.make_async_remote_copy(
            src_ref=CX.at[sp, :, mine],
            dst_ref=CX.at[slot, :, mine],
            send_sem=c_send.at[peer],
            recv_sem=c_recv.at[slot],
            device_id={"sp": peer},
            device_id_type=MESH,
        )

    def columns(piece, slot):
        span = pl.ds(piece * first_half, first_half)
        return CX.at[span, :, pl.ds(pl.multiple_of(slot * ft, ft), ft)]

    def x_copy(piece, peer, slot):
        return pltpu.make_async_remote_copy(
            src_ref=columns(piece, slot),
            dst_ref=columns(piece, slot),
            send_sem=x_send.at[piece * n_tp + peer],
            recv_sem=x_recv.at[piece * n_tp + slot],
            device_id={"tp": peer},
            device_id_type=MESH,
        )

    def d_copy(piece, slot, at):
        return pltpu.make_async_remote_copy(
            src_ref=columns(piece, slot),
            dst_ref=columns(piece, slot),
            send_sem=d_send.at[piece * n_tp + at],
            recv_sem=d_recv.at[piece * n_tp + at],
            device_id={"tp": partner},
            device_id_type=MESH,
        )

    chips = n_tp // 2

    def far(k):
        return lax.rem(tp + 2 * k, n_tp)

    @pl.when(sp > 0)
    def _():
        p1_copy(sp).start()

    def tell(k, c):
        pl.semaphore_signal(ready.at[sp], inc=1, device_id={"sp": k}, device_id_type=MESH)
        return c

    def send_back(k, c):
        c_copy(k, sp).start()
        return c

    lax.fori_loop(0, sp, tell, 0)
    lax.fori_loop(0, sp, send_back, 0)

    prepare()

    def send_on(j, c):
        pl.semaphore_wait(ready.at[j], 1)
        c_copy(j, sp).start()
        return c

    def send_late(j, c):
        @pl.when(sp > 0)
        def _():
            pl.semaphore_wait(ready.at[j], 1)

        c_copy(j, sp).start()
        return c

    def arrive(j, c):
        @pl.when(j != sp)
        def _():
            c_copy(j, j).wait_recv()

        return c

    def pass_on(piece):
        lax.fori_loop(piece * first_half, (piece + 1) * first_half, arrive, 0)
        for k in range(1, chips):
            x_copy(piece, far(k), tp).start()
        d_copy(piece, tp, 0).start()

    def hand_over(piece):
        for k in range(1, chips):
            x_copy(piece, far(k), far(k)).wait_recv()
            d_copy(piece, far(k), k).start()

    @pl.when(sp < first_half)
    def _():
        lax.fori_loop(sp + 1, first_half, send_on, 0)
        pass_on(0)

    @pl.when(sp == 0)
    def _():
        def p1_wait(j, c):
            p1_copy(j).wait_recv()
            return c

        lax.fori_loop(1, n_sp, p1_wait, 0)
        P2[...] = jnp.sum(R1[...], axis=0)

    @pl.when(sp > 0)
    def _():
        t_copy(0).wait_recv()

    R2[tp] = P2[...]

    def p2_copy(k, slot):
        peer = lax.rem(tp + k, n_tp)
        return pltpu.make_async_remote_copy(
            src_ref=P2,
            dst_ref=R2.at[tp if slot is None else peer],
            send_sem=p2_send.at[peer],
            recv_sem=p2_recv.at[tp if slot is None else peer],
            device_id={"tp": peer},
            device_id_type=MESH,
        )

    def p2_start(k, c):
        p2_copy(k, None).start()
        return c

    lax.fori_loop(1, n_tp, p2_start, 0)

    @pl.when(sp == 0)
    def _():
        def early(j, c):
            t_copy(j).start()
            return c

        def late(j, c):
            pl.semaphore_wait(ready.at[j], 1)
            t_copy(j).start()
            return c

        lax.fori_loop(1, first_half, early, 0)
        lax.fori_loop(first_half, n_sp, late, 0)

    lax.fori_loop(jnp.maximum(sp + 1, first_half), n_sp, send_late, 0)

    @pl.when(sp >= first_half)
    def _():
        pass_on(0)

    pass_on(1)
    hand_over(0)

    def p2_wait(k, c):
        p2_copy(k, 1).wait_recv()
        return c

    lax.fori_loop(1, n_tp, p2_wait, 0)

    r32 = lax.broadcasted_iota(jnp.int32, (32, ft), 0)
    for t in range(n_tp):
        cols = pl.ds(t * ft, ft)
        quad = jnp.zeros((32, ft), f32)
        for r, row in ((0, 0), (2, 3)):
            shift = R2[t, row : row + 1, :]
            high = shift.astype(bf16).astype(f32)
            quad = jnp.where(r32 == r, high, jnp.where(r32 == r + 1, shift - high, quad))
        LH[:, cols] = quad.astype(bf16)
    side = dot(LH[...], W[...])
    add = side[0:1] + side[1:2]
    ctx_add = side[2:3] + side[3:4]

    halves = ft // LANES
    per_slab = width // LANES

    def factors(row):
        rows_ = [
            R2[t, row : row + 1, s * LANES : (s + 1) * LANES]
            for t in range(n_tp)
            for s in range(halves)
        ]
        return GN[...].astype(f32) * (1.0 + jnp.concatenate(rows_, axis=0))

    slabs = [factors(1), factors(4), jnp.zeros((LANES - 2 * per_slab, LANES), f32)]
    turned = jnp.concatenate(slabs, axis=0).T
    for k in range(per_slab):
        at = pl.ds(k * LANES, LANES)
        W2[at, :] = (W[at, :].astype(f32) * turned[:, k : k + 1]).astype(bf16)
        W3[at, :] = (
            W[at, pl.ds(att, 2 * att)].astype(f32) * turned[:, per_slab + k : per_slab + k + 1]
        ).astype(bf16)

    per_block = HALO * GRID_W
    steps = rows // HALO
    head0 = lax.broadcasted_iota(jnp.int32, (COL_BLOCK, LANES), 1) < HEAD_DIM

    def h_copy(side_):
        return pltpu.make_async_remote_copy(
            src_ref=HB.at[side_],
            dst_ref=HR.at[side_],
            send_sem=h_send.at[side_],
            recv_sem=h_recv.at[side_],
            device_id={"sp": lax.rem(sp + (1 if side_ == 0 else n_sp - 1), n_sp)},
            device_id_type=MESH,
        )

    def project(k, c):
        m = jnp.where(k == 0, 0, jnp.where(k == 1, steps - 1, k - 1))
        at = pl.ds(pl.multiple_of(m * per_block, per_block), per_block)
        acc = dot(X[at, :], W2[...])
        rs = RS[at, :]
        parts = [
            acc[:, p * att : (p + 1) * att] * rs + add[:, p * att : (p + 1) * att]
            for p in range(3)
        ]
        q = parts[0] * (HEAD_DIM**-0.5)
        for r in range(HALO):
            for b in range(BLOCKS):
                begin = r * GRID_W + b * COL_BLOCK
                piece = q[begin : begin + COL_BLOCK]
                QS[b, m * HALO + r, 0] = jnp.where(head0, piece, 0.0).astype(bf16)
                QS[b, m * HALO + r, 1] = jnp.where(head0, 0.0, piece).astype(bf16)
                begin = r * GRID_W + STARTS[b]
                KS[b, m * HALO + r + HALO] = parts[1][begin : begin + STRIP].astype(bf16)
                VS[b, m * HALO + r + HALO, :, pl.ds(0, LANES)] = parts[2][
                    begin : begin + STRIP
                ].astype(bf16)

        @pl.when(k < 2)
        def _():
            HB[1 - k, :, pl.ds(0, att)] = parts[1].astype(bf16)
            HB[1 - k, :, pl.ds(att, att)] = parts[2].astype(bf16)

        return c

    lax.fori_loop(0, 2, project, 0)

    @pl.when(sp < n_sp - 1)
    def _():
        h_copy(0).start()

    @pl.when(sp > 0)
    def _():
        h_copy(1).start()

    lax.fori_loop(2, 4, project, 0)
    hand_over(1)
    lax.fori_loop(4, steps, project, 0)

    for piece in range(2):
        for k in range(chips):
            d_copy(piece, lax.rem(partner + 2 * k, n_tp), k).wait_recv()
    ctx_rows = CX.shape[1]
    pairs = dot(CX[...].reshape(n_sp * ctx_rows, width), W3[...])
    for s in range(n_sp):
        x = CX[s].astype(f32)
        mean = jnp.sum(x * x, axis=1, keepdims=True) * (1.0 / width)
        own = pl.ds(s * ctx_rows, ctx_rows)
        pair = (
            pairs[s * ctx_rows : (s + 1) * ctx_rows] * lax.rsqrt(mean + EPS) + ctx_add[:, att:]
        ).astype(bf16)
        CK[own, :] = pair[:, :att]
        CV[own, pl.ds(0, att)] = pair[:, att:]

    loads[12].wait()

    def spread(side_):
        first = 0 if side_ == 0 else rows + HALO
        for r in range(HALO):
            pair = HR[side_, pl.ds(r * GRID_W, GRID_W), :].astype(f32)
            for b in range(BLOCKS):
                strip = pair[STARTS[b] : STARTS[b] + STRIP].astype(bf16)
                KS[b, first + r] = strip[:, :att]
                VS[b, first + r, :, pl.ds(0, LANES)] = strip[:, att:]

    def a_copy(c, slot):
        return pltpu.make_async_remote_copy(
            src_ref=AS.at[c],
            dst_ref=AR.at[tp if slot is None else c],
            send_sem=a_send.at[c],
            recv_sem=a_recv.at[tp if slot is None else c],
            device_id={"tp": c},
            device_id_type=MESH,
        )

    low = -(-HALO // crows)
    inner = n_tp - 2 * low
    outer = 2 * low

    def attend(k, carry):
        @pl.when(k == inner)
        def _():
            @pl.when(sp > 0)
            def _():
                h_copy(0).wait_recv()
                spread(0)

            @pl.when(sp < n_sp - 1)
            def _():
                h_copy(1).wait_recv()
                spread(1)

        e = lax.rem(tp + 1 + k, outer)
        c = jnp.where(
            k < inner, low + lax.rem(tp + k, inner), jnp.where(e < low, e, e + inner)
        )
        rv = jnp.where(
            (sp == 0) & (c < 2), c + 1, jnp.where((sp == n_sp - 1) & (c == n_tp - 1), 3, 0)
        )
        base = jnp.where(
            (rv == 1) | (rv == 2), HALO, jnp.where(rv == 3, rows + HALO - urows, c * crows)
        )
        for b in range(BLOCKS):
            q2 = QS[b, pl.ds(c * crows, crows)].reshape(qrows, LANES)
            ks = KS[b, pl.ds(base, urows)].reshape(ukeys, LANES)
            near = dot_nt(q2, ks)
            table = TB[rv, VARIANT[b], :, :, :, pl.ds(0, ukeys)].reshape(qrows, ukeys)
            near = near + table
            far = dot_nt(q2, CK[...])
            peak = jnp.maximum(
                jnp.max(near, axis=1, keepdims=True), jnp.max(far, axis=1, keepdims=True)
            )
            near = jnp.exp(near - peak).astype(bf16)
            far = jnp.exp(far - peak).astype(bf16)
            vs = VS[b, pl.ds(base, urows)].reshape(ukeys, 2 * LANES)
            both = dot(near, vs) + dot(far, CV[...])
            value = (both[:, :LANES] / both[:, LANES:]).reshape(crows, 2, COL_BLOCK, LANES)
            for i in range(crows):
                AS[c, pl.ds(i * GRID_W + b * COL_BLOCK, COL_BLOCK), :] = jnp.where(
                    head0, value[i, 0], value[i, 1]
                ).astype(bf16)

        @pl.when(c != tp)
        def _():
            a_copy(c, None).start()

        return carry

    lax.fori_loop(0, n_tp, attend, 0)

    AR[tp] = AS[tp]

    def a_wait(k, c):
        a_copy(lax.rem(tp + k, n_tp), 1).wait_recv()
        return c

    lax.fori_loop(1, n_tp, a_wait, 0)
    merged = jnp.concatenate([AR[t] for t in range(n_tp)], axis=1)
    own = pl.ds(pl.multiple_of(tp * share, share), share)
    stores = []
    for t in range(n_tp):
        cols = pl.ds(t * ft, ft)
        branch = dot(merged, WO[:, cols])
        OB[:, cols] = (X[own, cols].astype(f32) + R2[t, 2:3, :] * branch).astype(bf16)
        store = pltpu.make_async_copy(OB.at[:, cols], out.at[:, cols], o_sem.at[t])
        store.start()
        stores.append(store)

    @pl.when(sp > 0)
    def _():
        p1_copy(sp).wait_send()

    @pl.when(sp == 0)
    def _():
        def t_done(j, c):
            t_copy(j).wait_send()
            return c

        lax.fori_loop(1, n_sp, t_done, 0)

    def c_done(j, c):
        @pl.when(j != sp)
        def _():
            c_copy(j, sp).wait_send()

        return c

    lax.fori_loop(0, n_sp, c_done, 0)

    def p2_done(k, c):
        p2_copy(k, None).wait_send()
        a_copy(lax.rem(tp + k, n_tp), None).wait_send()
        return c

    lax.fori_loop(1, n_tp, p2_done, 0)
    for piece in range(2):
        d_copy(piece, tp, 0).wait_send()
        for k in range(1, chips):
            x_copy(piece, far(k), tp).wait_send()
            d_copy(piece, far(k), k).wait_send()

    @pl.when(sp < n_sp - 1)
    def _():
        h_copy(0).wait_send()

    @pl.when(sp > 0)
    def _():
        h_copy(1).wait_send()

    for store in stores:
        store.wait()


def local(n_sp, n_tp, *args):
    (
        latent,
        condition,
        context_tokens,
        context_condition,
        shift_weight,
        scale_weight,
        gate_weight,
        norm_gain,
        query_weight,
        key_weight,
        value_weight,
        out_weight,
        offset_bias,
    ) = args
    tokens, width = latent.shape
    inputs, ft = shift_weight.shape
    att = query_weight.shape[1]
    rows = tokens // GRID_W
    crows = rows // n_tp
    share = crows * GRID_W
    urows = crows + WIN_ROWS - 1
    ctx_rows = context_tokens.shape[0]
    table = -(-urows * STRIP // LANES) * LANES
    padded = rows + 2 * HALO
    operands = (
        latent,
        condition.reshape(n_sp, inputs),
        context_tokens,
        context_condition.reshape(n_sp, inputs),
        shift_weight,
        scale_weight,
        gate_weight,
        norm_gain.reshape(n_sp, inputs),
        query_weight,
        key_weight,
        value_weight,
        out_weight,
        jnp.transpose(offset_bias, (1, 0, 2)),
    )
    dma = pltpu.SemaphoreType.DMA
    scratch = [
        pltpu.VMEM((tokens, width), bf16),
        pltpu.VMEM((n_sp, inputs), bf16),
        pltpu.VMEM((n_sp, inputs), bf16),
        pltpu.VMEM((3, inputs, ft), bf16),
        pltpu.VMEM((n_sp, inputs), bf16),
        pltpu.VMEM((width, 3 * att), bf16),
        pltpu.VMEM((width, 3 * att), bf16),
        pltpu.VMEM(out_weight.shape, bf16),
        pltpu.VMEM((offset_bias.shape[1], 2, offset_bias.shape[2]), f32),
        pltpu.VMEM((2, 16, LANES), f32),
        pltpu.VMEM((3, 2, 2 * WIN_ROWS, COL_BLOCK, LANES), f32),
        pltpu.VMEM((4, 3, crows, 2, COL_BLOCK, table), f32),
        pltpu.VMEM((tokens, LANES), f32),
        pltpu.VMEM((8, ft), f32),
        pltpu.VMEM((n_sp, 8, ft), f32),
        pltpu.VMEM((8, ft), f32),
        pltpu.VMEM((n_tp, 8, ft), f32),
        pltpu.VMEM((32, width), bf16),
        pltpu.VMEM((width, 2 * att), bf16),
        pltpu.VMEM((n_sp, ctx_rows, width), bf16),
        pltpu.VMEM((n_sp * ctx_rows, att), bf16),
        pltpu.VMEM((n_sp * ctx_rows, 2 * LANES), bf16),
        pltpu.VMEM((BLOCKS, rows, 2, COL_BLOCK, LANES), bf16),
        pltpu.VMEM((BLOCKS, padded, STRIP, LANES), bf16),
        pltpu.VMEM((BLOCKS, padded, STRIP, 2 * LANES), bf16),
        pltpu.VMEM((2, HALO * GRID_W, 2 * att), bf16),
        pltpu.VMEM((2, HALO * GRID_W, 2 * att), bf16),
        pltpu.VMEM((n_tp, share, LANES), bf16),
        pltpu.VMEM((n_tp, share, LANES), bf16),
        pltpu.VMEM((share, width), bf16),
        dma((13,)),
        dma((n_sp,)),
        dma((n_sp,)),
        dma((n_tp,)),
        dma((n_tp,)),
        dma((n_sp,)),
        dma((n_sp,)),
        dma((2 * n_tp,)),
        dma((2 * n_tp,)),
        dma((2 * n_tp,)),
        dma((2 * n_tp,)),
        dma((n_sp,)),
        dma((1,)),
        pltpu.SemaphoreType.REGULAR((n_sp,)),
        dma((2,)),
        dma((2,)),
        dma((n_tp,)),
        dma((n_tp,)),
        dma((n_tp,)),
    ]
    return pl.pallas_call(
        functools.partial(kernel, n_sp, n_tp),
        out_shape=jax.ShapeDtypeStruct((share, width), bf16),
        in_specs=[pl.BlockSpec(memory_space=pl.ANY)] * len(operands),
        out_specs=pl.BlockSpec(memory_space=pl.ANY),
        scratch_shapes=scratch,
        compiler_params=pltpu.CompilerParams(
            collective_id=0, has_side_effects=True, vmem_limit_bytes=60 * 1024 * 1024
        ),
    )(*operands)


def solution(mesh):
    placed = (
        P(("grp", "sp"), None),
        P("grp"),
        P(("grp", "sp"), None),
        P(),
        P("sp", "tp"),
        P("sp", "tp"),
        P("sp", "tp"),
        P(),
        P(None, "tp"),
        P(None, "tp"),
        P(None, "tp"),
        P(),
        P("tp", None, None),
    )
    return jax.shard_map(
        functools.partial(local, mesh.shape["sp"], mesh.shape["tp"]),
        mesh=mesh,
        in_specs=placed,
        out_specs=P(("grp", "sp", "tp"), None),
        check_vma=False,
    )
```

```python
import functools

import jax
import jax.numpy as jnp
from jax import lax
from jax.experimental import pallas as pl
from jax.experimental.pallas import tpu as pltpu
from jax.sharding import PartitionSpec as P

HEAD_DIM = 64
GRID_W = 64
WIN_ROWS = 8
WIN_COLS = 16
COL_BLOCK = 16
STRIP = COL_BLOCK + WIN_COLS
BLOCKS = GRID_W // COL_BLOCK
HALO = WIN_ROWS // 2
STARTS = (0, 8, 24, 32)
VARIANT = (0, 1, 1, 2)
SHIFTS = (15, 7, -1)
LEADERS = 1
EPS = 1e-6
MASKED = -1e30
LANES = 128

bf16 = jnp.bfloat16
f32 = jnp.float32
MESH = pl.DeviceIdType.MESH


def dot(a, b):
    return jnp.dot(a, b, preferred_element_type=f32)


def dot_nt(a, b):
    return lax.dot_general(a, b, (((1,), (1,)), ((), ())), preferred_element_type=f32)


def kernel(
    n_sp,
    n_tp,
    latent,
    cond,
    ctx_tokens,
    ctx_cond,
    shift_w,
    scale_w,
    gate_w,
    gain,
    query_w,
    key_w,
    value_w,
    out_w,
    bias,
    out,
    X,
    CD,
    XD,
    MW,
    GN,
    W,
    W2,
    WO,
    BI,
    PAD,
    TP,
    TB,
    RS,
    P1,
    R1,
    P2,
    R2,
    LH,
    W3,
    CX,
    CK,
    CV,
    QS,
    KS,
    VS,
    HB,
    HR,
    AS,
    AR,
    load_sem,
    p1_send,
    p1_recv,
    p2_send,
    p2_recv,
    c_send,
    c_recv,
    x_send,
    x_recv,
    d_send,
    d_recv,
    t_send,
    t_recv,
    ready,
    h_send,
    h_recv,
    a_send,
    a_recv,
):
    sp = lax.axis_index("sp")
    tp = lax.axis_index("tp")
    tokens, width = X.shape
    ft = width // n_tp
    rows = tokens // GRID_W
    crows = rows // n_tp
    share = crows * GRID_W
    urows = crows + WIN_ROWS - 1
    ukeys = urows * STRIP
    qrows = crows * 2 * COL_BLOCK
    att = W.shape[1] // 3

    barrier = pltpu.get_barrier_semaphore()

    def greet_sp(j, c):
        pl.semaphore_signal(barrier, inc=1, device_id={"sp": j}, device_id_type=MESH)
        return c

    def greet_tp(k, c):
        pl.semaphore_signal(
            barrier, inc=1, device_id={"tp": lax.rem(tp + k, n_tp)}, device_id_type=MESH
        )
        return c

    lax.fori_loop(sp + 1, n_sp, greet_sp, 0)
    lax.fori_loop(1, n_tp, greet_tp, 0)

    mine = pl.ds(pl.multiple_of(tp * ft, ft), ft)
    loads = [
        (shift_w, MW.at[0]),
        (scale_w, MW.at[1]),
        (gate_w, MW.at[2]),
        (cond, CD),
        (ctx_cond, XD),
        (ctx_tokens.at[:, mine], CX.at[sp, :, mine]),
        (bias, BI),
        (gain, GN),
        (latent, X),
        (query_w, W.at[:, pl.ds(0, att)]),
        (key_w, W.at[:, pl.ds(att, att)]),
        (value_w, W.at[:, pl.ds(2 * att, att)]),
        (out_w, WO),
    ]
    loads = [
        pltpu.make_async_copy(src, dst, load_sem.at[i]) for i, (src, dst) in enumerate(loads)
    ]
    for copy in loads:
        copy.start()

    row8 = lax.broadcasted_iota(jnp.int32, (8, ft), 0)

    for copy in loads[:5]:
        copy.wait()

    def own_act(ref):
        v = ref[...].astype(f32)
        act = (v / (1.0 + jnp.exp(-v))).astype(bf16).astype(f32)
        own = lax.broadcasted_iota(jnp.int32, act.shape, 0) == sp
        return jnp.sum(jnp.where(own, act, 0.0), axis=0, keepdims=True)

    own_cond, own_ctx = own_act(CD), own_act(XD)
    r16 = lax.broadcasted_iota(jnp.int32, (16, own_cond.shape[1]), 0)
    acts = jnp.where(r16 == 0, own_cond, jnp.where(r16 == 1, own_ctx, 0.0)).astype(bf16)
    d_shift, d_scale, d_gate = dot(acts, MW[0]), dot(acts, MW[1]), dot(acts, MW[2])
    terms = (d_shift[0:1], d_scale[0:1], d_gate[0:1], d_shift[1:2], d_scale[1:2])
    packed = jnp.zeros((8, ft), f32)
    for i, term in enumerate(terms):
        packed = jnp.where(row8 == i, term, packed)
    P1[...] = packed
    R1[sp] = packed

    def lay_tables():
        loads[6].wait()
        lane = lax.broadcasted_iota(jnp.int32, (COL_BLOCK, LANES), 1)
        in_group = lax.rem(lane, STRIP)
        query = lax.broadcasted_iota(jnp.int32, (COL_BLOCK, LANES), 0)
        lower = (
            jnp.maximum(query - WIN_COLS // 2, 0),
            query,
            jnp.minimum(query + WIN_COLS // 2, WIN_COLS),
        )
        inside = [(in_group >= lo) & (in_group < lo + WIN_COLS) for lo in lower]
        offsets = 2 * WIN_ROWS - 1
        PAD[...] = jnp.zeros_like(PAD)
        for h in range(2):
            PAD[h, pl.ds(0, offsets), pl.ds(0, 2 * WIN_COLS - 1)] = BI[:, h]
            x = PAD[h]
            x = x + pltpu.roll(x, 32, 1)
            PAD[h] = x + pltpu.roll(x, 64, 1)

        def lay_out(o, c):
            for h in range(2):
                line = jnp.broadcast_to(PAD[h, pl.ds(o, 1), :], (COL_BLOCK, LANES))
                for v in range(3):
                    turned = pltpu.roll(line, (-SHIFTS[v]) % LANES, 1, stride=1, stride_axis=0)
                    TP[v, h, o] = jnp.where(inside[v], turned, MASKED)
            return c

        lax.fori_loop(0, offsets, lay_out, 0)
        group = lane // STRIP
        per = LANES // STRIP
        variants = (
            (-HALO, lambda i: i),
            (0, lambda i: 0),
            (-crows, lambda i: max(crows + i - HALO, 0)),
            (-(urows - crows), lambda i: urows - WIN_ROWS),
        )

        def assemble(vh, c):
            v, h = vh // 2, lax.rem(vh, 2)
            for rv, (delta, first) in enumerate(variants):
                for i in range(crows):
                    for g in range(TB.shape[-1] // LANES):
                        tile = jnp.full((COL_BLOCK, LANES), MASKED, f32)
                        for l in range(per):
                            j = g * per + l
                            if first(i) <= j < first(i) + WIN_ROWS and j < urows:
                                o = delta + j - i + WIN_ROWS - 1
                                tile = jnp.where(group == l, TP[v, h, o], tile)
                        TB[rv, v, i, h, :, pl.ds(g * LANES, LANES)] = tile
            return c

        lax.fori_loop(0, 6, assemble, 0)


    def prepare():
        loads[8].wait()

        def norms(k, c):
            for u in range(4):
                at = pl.ds(pl.multiple_of(k * 64 + u * 16, 16), 16)
                x = X[at, :].astype(f32)
                mean = jnp.sum(x * x, axis=1, keepdims=True) * (1.0 / width)
                RS[at, :] = jnp.broadcast_to(lax.rsqrt(mean + EPS), (16, LANES))
            return c

        lax.fori_loop(0, tokens // 64, norms, 0)
        loads[7].wait()
        for copy in loads[9:12]:
            copy.wait()

        CV[:, pl.ds(LANES, LANES)] = jnp.ones((CV.shape[0], LANES), bf16)

        def fill(r, c):
            for b in range(BLOCKS):
                VS[b, r, :, pl.ds(LANES, LANES)] = jnp.ones((STRIP, LANES), bf16)
            return c

        lax.fori_loop(0, rows + 2 * HALO, fill, 0)

    loads[5].wait()
    pl.semaphore_wait(barrier, sp + n_tp - 1)
    first_half = n_sp // 2
    partner = tp + 1 - 2 * lax.rem(tp, 2)

    def p1_copy(peer, source):
        return pltpu.make_async_remote_copy(
            src_ref=P1,
            dst_ref=R1.at[source],
            send_sem=p1_send.at[peer],
            recv_sem=p1_recv.at[source],
            device_id={"sp": peer},
            device_id_type=MESH,
        )

    def t_copy(peer):
        return pltpu.make_async_remote_copy(
            src_ref=P2,
            dst_ref=P2,
            send_sem=t_send.at[peer],
            recv_sem=t_recv.at[0],
            device_id={"sp": peer},
            device_id_type=MESH,
        )

    def c_copy(peer, slot):
        return pltpu.make_async_remote_copy(
            src_ref=CX.at[sp, :, mine],
            dst_ref=CX.at[slot, :, mine],
            send_sem=c_send.at[peer],
            recv_sem=c_recv.at[slot],
            device_id={"sp": peer},
            device_id_type=MESH,
        )

    def columns(piece, slot):
        span = pl.ds(piece * first_half, first_half)
        return CX.at[span, :, pl.ds(pl.multiple_of(slot * ft, ft), ft)]

    def x_copy(piece, peer, slot):
        return pltpu.make_async_remote_copy(
            src_ref=columns(piece, slot),
            dst_ref=columns(piece, slot),
            send_sem=x_send.at[piece * n_tp + peer],
            recv_sem=x_recv.at[piece * n_tp + slot],
            device_id={"tp": peer},
            device_id_type=MESH,
        )

    def d_copy(piece, slot, at):
        return pltpu.make_async_remote_copy(
            src_ref=columns(piece, slot),
            dst_ref=columns(piece, slot),
            send_sem=d_send.at[piece * n_tp + at],
            recv_sem=d_recv.at[piece * n_tp + at],
            device_id={"tp": partner},
            device_id_type=MESH,
        )

    chips = n_tp // 2

    def far(k):
        return lax.rem(tp + 2 * k, n_tp)

    for leader in range(LEADERS):

        @pl.when(sp > leader)
        def _(leader=leader):
            p1_copy(leader, sp).start()

    def tell(k, c):
        pl.semaphore_signal(ready.at[sp], inc=1, device_id={"sp": k}, device_id_type=MESH)
        return c

    def send_back(k, c):
        c_copy(k, sp).start()
        return c

    lax.fori_loop(0, sp, tell, 0)
    lay_tables()
    lax.fori_loop(0, sp, send_back, 0)
    prepare()

    middle = 5 * n_sp // 8
    leads = sp < LEADERS
    if LEADERS == 1:
        middle = n_sp
    begins = jnp.where(sp == LEADERS - 1, LEADERS, jnp.where(sp == 0, middle, n_sp))
    ends = jnp.where(sp == LEADERS - 1, middle, n_sp)

    def send_on(j, c):
        pl.semaphore_wait(ready.at[j], 1)

        @pl.when(leads & (j < LEADERS))
        def _():
            p1_copy(j, sp).start()

        c_copy(j, sp).start()
        return c

    def send_late(j, c):
        @pl.when((j < begins) | (j >= ends))
        def _():
            pl.semaphore_wait(ready.at[j], 1)

        c_copy(j, sp).start()
        return c

    def arrive(j, c):
        @pl.when(j != sp)
        def _():
            c_copy(j, j).wait_recv()

        return c

    def pass_on(piece):
        lax.fori_loop(piece * first_half, (piece + 1) * first_half, arrive, 0)
        for k in range(1, chips):
            x_copy(piece, far(k), tp).start()
        d_copy(piece, tp, 0).start()

    def hand_over(piece):
        for k in range(1, chips):
            x_copy(piece, far(k), far(k)).wait_recv()
            d_copy(piece, far(k), k).start()

    @pl.when(sp < first_half)
    def _():
        lax.fori_loop(sp + 1, first_half, send_on, 0)

    @pl.when((sp < first_half) & jnp.logical_not(leads))
    def _():
        pass_on(0)

    @pl.when(leads)
    def _():
        def p1_wait(j, c):
            @pl.when(j != sp)
            def _():
                p1_copy(j, j).wait_recv()

            return c

        lax.fori_loop(0, n_sp, p1_wait, 0)
        P2[...] = jnp.sum(R1[...], axis=0)

    @pl.when(jnp.logical_not(leads))
    def _():
        t_copy(0).wait_recv()

    R2[tp] = P2[...]

    def p2_copy(k, slot):
        peer = lax.rem(tp + k, n_tp)
        return pltpu.make_async_remote_copy(
            src_ref=P2,
            dst_ref=R2.at[tp if slot is None else peer],
            send_sem=p2_send.at[peer],
            recv_sem=p2_recv.at[tp if slot is None else peer],
            device_id={"tp": peer},
            device_id_type=MESH,
        )

    def p2_start(k, c):
        p2_copy(k, None).start()
        return c

    lax.fori_loop(1, n_tp, p2_start, 0)

    def share_sums(j, c):
        @pl.when(j >= first_half)
        def _():
            pl.semaphore_wait(ready.at[j], 1)

        t_copy(j).start()
        return c

    lax.fori_loop(begins, ends, share_sums, 0)
    lax.fori_loop(jnp.maximum(sp + 1, first_half), n_sp, send_late, 0)

    @pl.when((sp >= first_half) | leads)
    def _():
        pass_on(0)

    pass_on(1)

    def p2_wait(k, c):
        p2_copy(k, 1).wait_recv()
        return c

    lax.fori_loop(1, n_tp, p2_wait, 0)

    r32 = lax.broadcasted_iota(jnp.int32, (32, ft), 0)
    for t in range(n_tp):
        cols = pl.ds(t * ft, ft)
        quad = jnp.zeros((32, ft), f32)
        for r, row in ((0, 0), (2, 3)):
            shift = R2[t, row : row + 1, :]
            high = shift.astype(bf16).astype(f32)
            quad = jnp.where(r32 == r, high, jnp.where(r32 == r + 1, shift - high, quad))
        LH[:, cols] = quad.astype(bf16)
    side = dot(LH[...], W[...])
    add = side[0:1] + side[1:2]
    ctx_add = side[2:3] + side[3:4]

    halves = ft // LANES
    per_slab = width // LANES

    def factors(row):
        rows_ = [
            R2[t, row : row + 1, s * LANES : (s + 1) * LANES]
            for t in range(n_tp)
            for s in range(halves)
        ]
        return GN[...].astype(f32) * (1.0 + jnp.concatenate(rows_, axis=0))

    slabs = [factors(1), factors(4), jnp.zeros((LANES - 2 * per_slab, LANES), f32)]
    turned = jnp.concatenate(slabs, axis=0).T
    for k in range(per_slab):
        at = pl.ds(k * LANES, LANES)
        W2[at, :] = (W[at, :].astype(f32) * turned[:, k : k + 1]).astype(bf16)
        W3[at, :] = (
            W[at, pl.ds(att, 2 * att)].astype(f32) * turned[:, per_slab + k : per_slab + k + 1]
        ).astype(bf16)

    hand_over(0)

    per_block = HALO * GRID_W
    steps = rows // HALO
    head0 = lax.broadcasted_iota(jnp.int32, (COL_BLOCK, LANES), 1) < HEAD_DIM

    def h_copy(side_):
        return pltpu.make_async_remote_copy(
            src_ref=HB.at[side_],
            dst_ref=HR.at[side_],
            send_sem=h_send.at[side_],
            recv_sem=h_recv.at[side_],
            device_id={"sp": lax.rem(sp + (1 if side_ == 0 else n_sp - 1), n_sp)},
            device_id_type=MESH,
        )

    def project(k, c):
        m = jnp.where(k == 0, 0, jnp.where(k == 1, steps - 1, k - 1))
        at = pl.ds(pl.multiple_of(m * per_block, per_block), per_block)
        acc = dot(X[at, :], W2[...])
        rs = RS[at, :]
        parts = [
            acc[:, p * att : (p + 1) * att] * rs + add[:, p * att : (p + 1) * att]
            for p in range(3)
        ]
        q = parts[0] * (HEAD_DIM**-0.5)
        for r in range(HALO):
            for b in range(BLOCKS):
                begin = r * GRID_W + b * COL_BLOCK
                piece = q[begin : begin + COL_BLOCK]
                QS[b, m * HALO + r, 0] = jnp.where(head0, piece, 0.0).astype(bf16)
                QS[b, m * HALO + r, 1] = jnp.where(head0, 0.0, piece).astype(bf16)
                begin = r * GRID_W + STARTS[b]
                KS[b, m * HALO + r + HALO] = parts[1][begin : begin + STRIP].astype(bf16)
                VS[b, m * HALO + r + HALO, :, pl.ds(0, LANES)] = parts[2][
                    begin : begin + STRIP
                ].astype(bf16)

        @pl.when(k < 2)
        def _():
            HB[1 - k, :, pl.ds(0, att)] = parts[1].astype(bf16)
            HB[1 - k, :, pl.ds(att, att)] = parts[2].astype(bf16)

        return c

    lax.fori_loop(0, 2, project, 0)

    @pl.when(sp < n_sp - 1)
    def _():
        h_copy(0).start()

    @pl.when(sp > 0)
    def _():
        h_copy(1).start()

    lax.fori_loop(2, 4, project, 0)
    hand_over(1)
    lax.fori_loop(4, steps, project, 0)

    for piece in range(2):
        for k in range(chips):
            d_copy(piece, lax.rem(partner + 2 * k, n_tp), k).wait_recv()
    ctx_rows = CX.shape[1]
    pairs = dot(CX[...].reshape(n_sp * ctx_rows, width), W3[...])
    for s in range(n_sp):
        x = CX[s].astype(f32)
        mean = jnp.sum(x * x, axis=1, keepdims=True) * (1.0 / width)
        own = pl.ds(s * ctx_rows, ctx_rows)
        pair = (
            pairs[s * ctx_rows : (s + 1) * ctx_rows] * lax.rsqrt(mean + EPS) + ctx_add[:, att:]
        ).astype(bf16)
        CK[own, :] = pair[:, :att]
        CV[own, pl.ds(0, att)] = pair[:, att:]

    loads[12].wait()

    def spread(side_):
        first = 0 if side_ == 0 else rows + HALO
        for r in range(HALO):
            pair = HR[side_, pl.ds(r * GRID_W, GRID_W), :].astype(f32)
            for b in range(BLOCKS):
                strip = pair[STARTS[b] : STARTS[b] + STRIP].astype(bf16)
                KS[b, first + r] = strip[:, :att]
                VS[b, first + r, :, pl.ds(0, LANES)] = strip[:, att:]

    def a_copy(c, slot):
        return pltpu.make_async_remote_copy(
            src_ref=AS.at[c],
            dst_ref=AR.at[tp if slot is None else c],
            send_sem=a_send.at[c],
            recv_sem=a_recv.at[tp if slot is None else c],
            device_id={"tp": c},
            device_id_type=MESH,
        )

    low = -(-HALO // crows)
    inner = n_tp - 2 * low
    outer = 2 * low

    def attend(k, carry):
        @pl.when(k == inner)
        def _():
            @pl.when(sp > 0)
            def _():
                h_copy(0).wait_recv()
                spread(0)

            @pl.when(sp < n_sp - 1)
            def _():
                h_copy(1).wait_recv()
                spread(1)

        e = lax.rem(tp + 1 + k, outer)
        c = jnp.where(
            k < inner, low + lax.rem(tp + k, inner), jnp.where(e < low, e, e + inner)
        )
        rv = jnp.where(
            (sp == 0) & (c < 2), c + 1, jnp.where((sp == n_sp - 1) & (c == n_tp - 1), 3, 0)
        )
        base = jnp.where(
            (rv == 1) | (rv == 2), HALO, jnp.where(rv == 3, rows + HALO - urows, c * crows)
        )
        qs = [QS[b, pl.ds(c * crows, crows)].reshape(qrows, LANES) for b in range(BLOCKS)]
        fars = dot_nt(jnp.concatenate(qs, axis=0), CK[...])
        near_exps, far_exps = [], []
        for b in range(BLOCKS):
            ks = KS[b, pl.ds(base, urows)].reshape(ukeys, LANES)
            table = TB[rv, VARIANT[b], :, :, :, pl.ds(0, ukeys)].reshape(qrows, ukeys)
            near = dot_nt(qs[b], ks) + table
            far = fars[b * qrows : (b + 1) * qrows]
            peak = jnp.maximum(
                jnp.max(near, axis=1, keepdims=True), jnp.max(far, axis=1, keepdims=True)
            )
            near_exps.append(jnp.exp(near - peak).astype(bf16))
            far_exps.append(jnp.exp(far - peak).astype(bf16))
        far_sums = dot(jnp.concatenate(far_exps, axis=0), CV[...])
        for b in range(BLOCKS):
            vs = VS[b, pl.ds(base, urows)].reshape(ukeys, 2 * LANES)
            both = dot(near_exps[b], vs) + far_sums[b * qrows : (b + 1) * qrows]
            value = (both[:, :LANES] / both[:, LANES:]).reshape(crows, 2, COL_BLOCK, LANES)
            for i in range(crows):
                AS[c, pl.ds(i * GRID_W + b * COL_BLOCK, COL_BLOCK), :] = jnp.where(
                    head0, value[i, 0], value[i, 1]
                ).astype(bf16)

        @pl.when(c != tp)
        def _():
            a_copy(c, None).start()

        return carry

    lax.fori_loop(0, n_tp, attend, 0)

    AR[tp] = AS[tp]

    def a_wait(k, c):
        a_copy(lax.rem(tp + k, n_tp), 1).wait_recv()
        return c

    lax.fori_loop(1, n_tp, a_wait, 0)
    merged = jnp.concatenate([AR[t] for t in range(n_tp)], axis=1)
    own = pl.ds(pl.multiple_of(tp * share, share), share)
    for t in range(n_tp):
        cols = pl.ds(t * ft, ft)
        branch = dot(merged, WO[:, cols])
        out[:, cols] = (X[own, cols].astype(f32) + R2[t, 2:3, :] * branch).astype(bf16)

    def p1_done(j, c):
        @pl.when(j != sp)
        def _():
            p1_copy(j, sp).wait_send()

        return c

    lax.fori_loop(0, LEADERS, p1_done, 0)

    def t_done(j, c):
        t_copy(j).wait_send()
        return c

    lax.fori_loop(begins, ends, t_done, 0)

    def c_done(j, c):
        @pl.when(j != sp)
        def _():
            c_copy(j, sp).wait_send()

        return c

    lax.fori_loop(0, n_sp, c_done, 0)

    def p2_done(k, c):
        p2_copy(k, None).wait_send()
        a_copy(lax.rem(tp + k, n_tp), None).wait_send()
        return c

    lax.fori_loop(1, n_tp, p2_done, 0)
    for piece in range(2):
        d_copy(piece, tp, 0).wait_send()
        for k in range(1, chips):
            x_copy(piece, far(k), tp).wait_send()
            d_copy(piece, far(k), k).wait_send()

    @pl.when(sp < n_sp - 1)
    def _():
        h_copy(0).wait_send()

    @pl.when(sp > 0)
    def _():
        h_copy(1).wait_send()


def local(n_sp, n_tp, *args):
    (
        latent,
        condition,
        context_tokens,
        context_condition,
        shift_weight,
        scale_weight,
        gate_weight,
        norm_gain,
        query_weight,
        key_weight,
        value_weight,
        out_weight,
        offset_bias,
    ) = args
    tokens, width = latent.shape
    inputs, ft = shift_weight.shape
    att = query_weight.shape[1]
    rows = tokens // GRID_W
    crows = rows // n_tp
    share = crows * GRID_W
    urows = crows + WIN_ROWS - 1
    ctx_rows = context_tokens.shape[0]
    table = -(-urows * STRIP // LANES) * LANES
    padded = rows + 2 * HALO
    operands = (
        latent,
        condition.reshape(n_sp, inputs),
        context_tokens,
        context_condition.reshape(n_sp, inputs),
        shift_weight,
        scale_weight,
        gate_weight,
        norm_gain.reshape(n_sp, inputs),
        query_weight,
        key_weight,
        value_weight,
        out_weight,
        jnp.transpose(offset_bias, (1, 0, 2)),
    )
    dma = pltpu.SemaphoreType.DMA
    scratch = [
        pltpu.VMEM((tokens, width), bf16),
        pltpu.VMEM((n_sp, inputs), bf16),
        pltpu.VMEM((n_sp, inputs), bf16),
        pltpu.VMEM((3, inputs, ft), bf16),
        pltpu.VMEM((n_sp, inputs), bf16),
        pltpu.VMEM((width, 3 * att), bf16),
        pltpu.VMEM((width, 3 * att), bf16),
        pltpu.VMEM(out_weight.shape, bf16),
        pltpu.VMEM((offset_bias.shape[1], 2, offset_bias.shape[2]), f32),
        pltpu.VMEM((2, 16, LANES), f32),
        pltpu.VMEM((3, 2, 2 * WIN_ROWS, COL_BLOCK, LANES), f32),
        pltpu.VMEM((4, 3, crows, 2, COL_BLOCK, table), f32),
        pltpu.VMEM((tokens, LANES), f32),
        pltpu.VMEM((8, ft), f32),
        pltpu.VMEM((n_sp, 8, ft), f32),
        pltpu.VMEM((8, ft), f32),
        pltpu.VMEM((n_tp, 8, ft), f32),
        pltpu.VMEM((32, width), bf16),
        pltpu.VMEM((width, 2 * att), bf16),
        pltpu.VMEM((n_sp, ctx_rows, width), bf16),
        pltpu.VMEM((n_sp * ctx_rows, att), bf16),
        pltpu.VMEM((n_sp * ctx_rows, 2 * LANES), bf16),
        pltpu.VMEM((BLOCKS, rows, 2, COL_BLOCK, LANES), bf16),
        pltpu.VMEM((BLOCKS, padded, STRIP, LANES), bf16),
        pltpu.VMEM((BLOCKS, padded, STRIP, 2 * LANES), bf16),
        pltpu.VMEM((2, HALO * GRID_W, 2 * att), bf16),
        pltpu.VMEM((2, HALO * GRID_W, 2 * att), bf16),
        pltpu.VMEM((n_tp, share, LANES), bf16),
        pltpu.VMEM((n_tp, share, LANES), bf16),
        dma((13,)),
        dma((n_sp,)),
        dma((n_sp,)),
        dma((n_tp,)),
        dma((n_tp,)),
        dma((n_sp,)),
        dma((n_sp,)),
        dma((2 * n_tp,)),
        dma((2 * n_tp,)),
        dma((2 * n_tp,)),
        dma((2 * n_tp,)),
        dma((n_sp,)),
        dma((1,)),
        pltpu.SemaphoreType.REGULAR((n_sp,)),
        dma((2,)),
        dma((2,)),
        dma((n_tp,)),
        dma((n_tp,)),
    ]
    operands = tuple(pltpu.with_memory_space_constraint(x, pltpu.HBM) for x in operands)
    return pl.pallas_call(
        functools.partial(kernel, n_sp, n_tp),
        out_shape=jax.ShapeDtypeStruct((share, width), bf16),
        in_specs=[pl.BlockSpec(memory_space=pl.ANY)] * len(operands),
        out_specs=pl.BlockSpec(memory_space=pltpu.VMEM),
        scratch_shapes=scratch,
        compiler_params=pltpu.CompilerParams(
            collective_id=0, has_side_effects=True, vmem_limit_bytes=46_000_000
        ),
    )(*operands)


def solution(mesh):
    placed = (
        P(("grp", "sp"), None),
        P("grp"),
        P(("grp", "sp"), None),
        P(),
        P("sp", "tp"),
        P("sp", "tp"),
        P("sp", "tp"),
        P(),
        P(None, "tp"),
        P(None, "tp"),
        P(None, "tp"),
        P(),
        P("tp", None, None),
    )
    return jax.shard_map(
        functools.partial(local, mesh.shape["sp"], mesh.shape["tp"]),
        mesh=mesh,
        in_specs=placed,
        out_specs=P(("grp", "sp", "tp"), None),
        check_vma=False,
    )
```

```python
import functools

import jax
import jax.numpy as jnp
from jax import lax
from jax.experimental import pallas as pl
from jax.experimental.pallas import tpu as pltpu
from jax.sharding import PartitionSpec as P

HEAD_DIM = 64
GRID_W = 64
WIN_ROWS = 8
WIN_COLS = 16
COL_BLOCK = 16
STRIP = COL_BLOCK + WIN_COLS
BLOCKS = GRID_W // COL_BLOCK
HALO = WIN_ROWS // 2
STARTS = (0, 8, 24, 32)
VARIANT = (0, 1, 1, 2)
SHIFTS = (15, 7, -1)
LEADERS = 1
EPS = 1e-6
MASKED = -1e30
LANES = 128

bf16 = jnp.bfloat16
f32 = jnp.float32
MESH = pl.DeviceIdType.MESH


def dot(a, b):
    return jnp.dot(a, b, preferred_element_type=f32)


def dot_nt(a, b):
    return lax.dot_general(a, b, (((1,), (1,)), ((), ())), preferred_element_type=f32)


def kernel(
    n_sp,
    n_tp,
    latent,
    cond,
    ctx_tokens,
    ctx_cond,
    shift_w,
    scale_w,
    gate_w,
    gain,
    query_w,
    key_w,
    value_w,
    out_w,
    bias,
    out,
    X,
    CD,
    XD,
    MW,
    GN,
    W,
    W2,
    WO,
    BI,
    PAD,
    TP,
    TB,
    RS,
    P1,
    R1,
    P2,
    R2,
    LH,
    W3,
    CX,
    CK,
    CV,
    QS,
    KS,
    VS,
    HB,
    HR,
    AS,
    AR,
    load_sem,
    p1_send,
    p1_recv,
    p2_send,
    p2_recv,
    c_send,
    c_recv,
    x_send,
    x_recv,
    d_send,
    d_recv,
    t_send,
    t_recv,
    ready,
    h_send,
    h_recv,
    a_send,
    a_recv,
):
    sp = lax.axis_index("sp")
    tp = lax.axis_index("tp")
    tokens, width = X.shape
    ft = width // n_tp
    rows = tokens // GRID_W
    crows = rows // n_tp
    share = crows * GRID_W
    urows = crows + WIN_ROWS - 1
    ukeys = urows * STRIP
    qrows = crows * 2 * COL_BLOCK
    att = W.shape[1] // 3

    barrier = pltpu.get_barrier_semaphore()

    def greet_sp(j, c):
        pl.semaphore_signal(barrier, inc=1, device_id={"sp": j}, device_id_type=MESH)
        return c

    def greet_tp(k, c):
        pl.semaphore_signal(
            barrier, inc=1, device_id={"tp": lax.rem(tp + k, n_tp)}, device_id_type=MESH
        )
        return c

    lax.fori_loop(sp + 1, n_sp, greet_sp, 0)
    lax.fori_loop(1, n_tp, greet_tp, 0)

    mine = pl.ds(pl.multiple_of(tp * ft, ft), ft)
    loads = [
        (shift_w, MW.at[0]),
        (scale_w, MW.at[1]),
        (gate_w, MW.at[2]),
        (cond, CD),
        (ctx_cond, XD),
        (ctx_tokens.at[:, mine], CX.at[sp, :, mine]),
        (bias, BI),
        (gain, GN),
        (latent, X),
        (query_w, W.at[:, pl.ds(0, att)]),
        (key_w, W.at[:, pl.ds(att, att)]),
        (value_w, W.at[:, pl.ds(2 * att, att)]),
        (out_w, WO),
    ]
    loads = [
        pltpu.make_async_copy(src, dst, load_sem.at[i]) for i, (src, dst) in enumerate(loads)
    ]
    for copy in loads:
        copy.start()

    row8 = lax.broadcasted_iota(jnp.int32, (8, ft), 0)

    for copy in loads[:5]:
        copy.wait()

    def own_act(ref):
        v = ref[...].astype(f32)
        act = (v / (1.0 + jnp.exp(-v))).astype(bf16).astype(f32)
        own = lax.broadcasted_iota(jnp.int32, act.shape, 0) == sp
        return jnp.sum(jnp.where(own, act, 0.0), axis=0, keepdims=True)

    own_cond, own_ctx = own_act(CD), own_act(XD)
    r16 = lax.broadcasted_iota(jnp.int32, (16, own_cond.shape[1]), 0)
    acts = jnp.where(r16 == 0, own_cond, jnp.where(r16 == 1, own_ctx, 0.0)).astype(bf16)
    d_shift, d_scale, d_gate = dot(acts, MW[0]), dot(acts, MW[1]), dot(acts, MW[2])
    terms = (d_shift[0:1], d_scale[0:1], d_gate[0:1], d_shift[1:2], d_scale[1:2])
    packed = jnp.zeros((8, ft), f32)
    for i, term in enumerate(terms):
        packed = jnp.where(row8 == i, term, packed)
    P1[...] = packed
    R1[sp] = packed

    def lay_tables():
        loads[6].wait()
        lane = lax.broadcasted_iota(jnp.int32, (COL_BLOCK, LANES), 1)
        in_group = lax.rem(lane, STRIP)
        query = lax.broadcasted_iota(jnp.int32, (COL_BLOCK, LANES), 0)
        lower = (
            jnp.maximum(query - WIN_COLS // 2, 0),
            query,
            jnp.minimum(query + WIN_COLS // 2, WIN_COLS),
        )
        inside = [(in_group >= lo) & (in_group < lo + WIN_COLS) for lo in lower]
        offsets = 2 * WIN_ROWS - 1
        PAD[...] = jnp.zeros_like(PAD)
        for h in range(2):
            PAD[h, pl.ds(0, offsets), pl.ds(0, 2 * WIN_COLS - 1)] = BI[:, h]
            x = PAD[h]
            x = x + pltpu.roll(x, 32, 1)
            PAD[h] = x + pltpu.roll(x, 64, 1)

        def lay_out(o, c):
            for h in range(2):
                line = jnp.broadcast_to(PAD[h, pl.ds(o, 1), :], (COL_BLOCK, LANES))
                for v in range(3):
                    turned = pltpu.roll(line, (-SHIFTS[v]) % LANES, 1, stride=1, stride_axis=0)
                    TP[v, h, o] = jnp.where(inside[v], turned, MASKED)
            return c

        lax.fori_loop(0, offsets, lay_out, 0)
        group = lane // STRIP
        per = LANES // STRIP
        variants = (
            (-HALO, lambda i: i),
            (0, lambda i: 0),
            (-crows, lambda i: max(crows + i - HALO, 0)),
            (-(urows - crows), lambda i: urows - WIN_ROWS),
        )

        def assemble(vh, c):
            v, h = vh // 2, lax.rem(vh, 2)
            for rv, (delta, first) in enumerate(variants):
                for i in range(crows):
                    for g in range(TB.shape[-1] // LANES):
                        tile = jnp.full((COL_BLOCK, LANES), MASKED, f32)
                        for l in range(per):
                            j = g * per + l
                            if first(i) <= j < first(i) + WIN_ROWS and j < urows:
                                o = delta + j - i + WIN_ROWS - 1
                                tile = jnp.where(group == l, TP[v, h, o], tile)
                        TB[rv, v, i, h, :, pl.ds(g * LANES, LANES)] = tile
            return c

        lax.fori_loop(0, 6, assemble, 0)


    def prepare():
        loads[8].wait()

        def norms(k, c):
            for u in range(4):
                at = pl.ds(pl.multiple_of(k * 64 + u * 16, 16), 16)
                x = X[at, :].astype(f32)
                mean = jnp.sum(x * x, axis=1, keepdims=True) * (1.0 / width)
                RS[at, :] = jnp.broadcast_to(lax.rsqrt(mean + EPS), (16, LANES))
            return c

        lax.fori_loop(0, tokens // 64, norms, 0)
        loads[7].wait()
        for copy in loads[9:12]:
            copy.wait()

        CV[:, pl.ds(LANES, LANES)] = jnp.ones((CV.shape[0], LANES), bf16)

        def fill(r, c):
            for b in range(BLOCKS):
                VS[b, r, :, pl.ds(LANES, LANES)] = jnp.ones((STRIP, LANES), bf16)
            return c

        lax.fori_loop(0, rows + 2 * HALO, fill, 0)

    @pl.when(sp == 0)
    def _():
        lay_tables()
        prepare()

    loads[5].wait()
    pl.semaphore_wait(barrier, sp + n_tp - 1)
    first_half = n_sp // 2
    partner = tp + 1 - 2 * lax.rem(tp, 2)

    def p1_copy(peer, source):
        return pltpu.make_async_remote_copy(
            src_ref=P1,
            dst_ref=R1.at[source],
            send_sem=p1_send.at[peer],
            recv_sem=p1_recv.at[source],
            device_id={"sp": peer},
            device_id_type=MESH,
        )

    def t_copy(peer):
        return pltpu.make_async_remote_copy(
            src_ref=P2,
            dst_ref=P2,
            send_sem=t_send.at[peer],
            recv_sem=t_recv.at[0],
            device_id={"sp": peer},
            device_id_type=MESH,
        )

    def c_copy(peer, slot):
        return pltpu.make_async_remote_copy(
            src_ref=CX.at[sp, :, mine],
            dst_ref=CX.at[slot, :, mine],
            send_sem=c_send.at[peer],
            recv_sem=c_recv.at[slot],
            device_id={"sp": peer},
            device_id_type=MESH,
        )

    def columns(piece, slot):
        span = pl.ds(piece * first_half, first_half)
        return CX.at[span, :, pl.ds(pl.multiple_of(slot * ft, ft), ft)]

    def x_copy(piece, peer, slot):
        return pltpu.make_async_remote_copy(
            src_ref=columns(piece, slot),
            dst_ref=columns(piece, slot),
            send_sem=x_send.at[piece * n_tp + peer],
            recv_sem=x_recv.at[piece * n_tp + slot],
            device_id={"tp": peer},
            device_id_type=MESH,
        )

    def d_copy(piece, slot, at):
        return pltpu.make_async_remote_copy(
            src_ref=columns(piece, slot),
            dst_ref=columns(piece, slot),
            send_sem=d_send.at[piece * n_tp + at],
            recv_sem=d_recv.at[piece * n_tp + at],
            device_id={"tp": partner},
            device_id_type=MESH,
        )

    chips = n_tp // 2

    def far(k):
        return lax.rem(tp + 2 * k, n_tp)

    for leader in range(LEADERS):

        @pl.when(sp > leader)
        def _(leader=leader):
            p1_copy(leader, sp).start()

    def tell(k, c):
        pl.semaphore_signal(ready.at[sp], inc=1, device_id={"sp": k}, device_id_type=MESH)
        return c

    def send_back(k, c):
        c_copy(k, sp).start()
        return c

    lax.fori_loop(0, sp, tell, 0)
    @pl.when(sp > 0)
    def _():
        lay_tables()
        lax.fori_loop(0, sp, send_back, 0)
        prepare()

    middle = 5 * n_sp // 8
    leads = sp < LEADERS
    if LEADERS == 1:
        middle = n_sp
    begins = jnp.where(sp == LEADERS - 1, LEADERS, jnp.where(sp == 0, middle, n_sp))
    ends = jnp.where(sp == LEADERS - 1, middle, n_sp)

    def send_on(j, c):
        pl.semaphore_wait(ready.at[j], 1)

        @pl.when(leads & (j < LEADERS))
        def _():
            p1_copy(j, sp).start()

        c_copy(j, sp).start()
        return c

    def send_late(j, c):
        @pl.when((j < begins) | (j >= ends))
        def _():
            pl.semaphore_wait(ready.at[j], 1)

        c_copy(j, sp).start()
        return c

    def arrive(j, c):
        @pl.when(j != sp)
        def _():
            c_copy(j, j).wait_recv()

        return c

    def pass_on(piece):
        lax.fori_loop(piece * first_half, (piece + 1) * first_half, arrive, 0)
        for k in range(1, chips):
            x_copy(piece, far(k), tp).start()
        d_copy(piece, tp, 0).start()

    def hand_over(piece):
        for k in range(1, chips):
            x_copy(piece, far(k), far(k)).wait_recv()
            d_copy(piece, far(k), k).start()

    @pl.when(sp < first_half)
    def _():
        lax.fori_loop(sp + 1, first_half, send_on, 0)

    @pl.when((sp < first_half) & jnp.logical_not(leads))
    def _():
        pass_on(0)

    @pl.when(leads)
    def _():
        def p1_wait(j, c):
            @pl.when(j != sp)
            def _():
                p1_copy(j, j).wait_recv()

            return c

        lax.fori_loop(0, n_sp, p1_wait, 0)
        P2[...] = jnp.sum(R1[...], axis=0)

    @pl.when(jnp.logical_not(leads))
    def _():
        t_copy(0).wait_recv()

    R2[tp] = P2[...]

    def p2_copy(k, slot):
        peer = lax.rem(tp + k, n_tp)
        return pltpu.make_async_remote_copy(
            src_ref=P2,
            dst_ref=R2.at[tp if slot is None else peer],
            send_sem=p2_send.at[peer],
            recv_sem=p2_recv.at[tp if slot is None else peer],
            device_id={"tp": peer},
            device_id_type=MESH,
        )

    def p2_start(k, c):
        p2_copy(k, None).start()
        return c

    def share_sums(j, c):
        @pl.when(j >= first_half)
        def _():
            pl.semaphore_wait(ready.at[j], 1)

        t_copy(j).start()
        return c

    nearest = jnp.minimum(begins + 2, ends)
    lax.fori_loop(begins, nearest, share_sums, 0)
    lax.fori_loop(1, n_tp, p2_start, 0)

    lax.fori_loop(nearest, ends, share_sums, 0)
    lax.fori_loop(jnp.maximum(sp + 1, first_half), n_sp, send_late, 0)

    @pl.when((sp >= first_half) | leads)
    def _():
        pass_on(0)

    pass_on(1)

    def p2_wait(k, c):
        p2_copy(k, 1).wait_recv()
        return c

    lax.fori_loop(1, n_tp, p2_wait, 0)

    r32 = lax.broadcasted_iota(jnp.int32, (32, ft), 0)
    for t in range(n_tp):
        cols = pl.ds(t * ft, ft)
        quad = jnp.zeros((32, ft), f32)
        for r, row in ((0, 0), (2, 3)):
            shift = R2[t, row : row + 1, :]
            high = shift.astype(bf16).astype(f32)
            quad = jnp.where(r32 == r, high, jnp.where(r32 == r + 1, shift - high, quad))
        LH[:, cols] = quad.astype(bf16)
    side = dot(LH[...], W[...])
    add = side[0:1] + side[1:2]
    ctx_add = side[2:3] + side[3:4]

    halves = ft // LANES
    per_slab = width // LANES

    def factors(row):
        rows_ = [
            R2[t, row : row + 1, s * LANES : (s + 1) * LANES]
            for t in range(n_tp)
            for s in range(halves)
        ]
        return GN[...].astype(f32) * (1.0 + jnp.concatenate(rows_, axis=0))

    slabs = [factors(1), factors(4), jnp.zeros((LANES - 2 * per_slab, LANES), f32)]
    turned = jnp.concatenate(slabs, axis=0).T
    for k in range(per_slab):
        at = pl.ds(k * LANES, LANES)
        W2[at, :] = (W[at, :].astype(f32) * turned[:, k : k + 1]).astype(bf16)

    per_block = HALO * GRID_W
    steps = rows // HALO
    head0 = lax.broadcasted_iota(jnp.int32, (COL_BLOCK, LANES), 1) < HEAD_DIM

    def h_copy(side_):
        return pltpu.make_async_remote_copy(
            src_ref=HB.at[side_],
            dst_ref=HR.at[side_],
            send_sem=h_send.at[side_],
            recv_sem=h_recv.at[side_],
            device_id={"sp": lax.rem(sp + (1 if side_ == 0 else n_sp - 1), n_sp)},
            device_id_type=MESH,
        )

    def project(k, c):
        m = jnp.where(k == 0, 0, jnp.where(k == 1, steps - 1, k - 1))
        at = pl.ds(pl.multiple_of(m * per_block, per_block), per_block)
        acc = dot(X[at, :], W2[...])
        rs = RS[at, :]
        parts = [
            acc[:, p * att : (p + 1) * att] * rs + add[:, p * att : (p + 1) * att]
            for p in range(3)
        ]
        q = parts[0] * (HEAD_DIM**-0.5)
        for r in range(HALO):
            for b in range(BLOCKS):
                begin = r * GRID_W + b * COL_BLOCK
                piece = q[begin : begin + COL_BLOCK]
                QS[b, m * HALO + r, 0] = jnp.where(head0, piece, 0.0).astype(bf16)
                QS[b, m * HALO + r, 1] = jnp.where(head0, 0.0, piece).astype(bf16)
                begin = r * GRID_W + STARTS[b]
                KS[b, m * HALO + r + HALO] = parts[1][begin : begin + STRIP].astype(bf16)
                VS[b, m * HALO + r + HALO, :, pl.ds(0, LANES)] = parts[2][
                    begin : begin + STRIP
                ].astype(bf16)

        @pl.when(k < 2)
        def _():
            HB[1 - k, :, pl.ds(0, att)] = parts[1].astype(bf16)
            HB[1 - k, :, pl.ds(att, att)] = parts[2].astype(bf16)

        return c

    lax.fori_loop(0, 2, project, 0)

    @pl.when(sp < n_sp - 1)
    def _():
        h_copy(0).start()

    @pl.when(sp > 0)
    def _():
        h_copy(1).start()

    lax.fori_loop(2, steps - 2, project, 0)
    hand_over(0)
    lax.fori_loop(steps - 2, steps - 1, project, 0)
    hand_over(1)
    lax.fori_loop(steps - 1, steps, project, 0)

    for k in range(per_slab):
        at = pl.ds(k * LANES, LANES)
        W3[at, :] = (
            W[at, pl.ds(att, 2 * att)].astype(f32) * turned[:, per_slab + k : per_slab + k + 1]
        ).astype(bf16)

    for piece in range(2):
        for k in range(chips):
            d_copy(piece, lax.rem(partner + 2 * k, n_tp), k).wait_recv()
    ctx_rows = CX.shape[1]
    pairs = dot(CX[...].reshape(n_sp * ctx_rows, width), W3[...])
    for s in range(n_sp):
        x = CX[s].astype(f32)
        mean = jnp.sum(x * x, axis=1, keepdims=True) * (1.0 / width)
        own = pl.ds(s * ctx_rows, ctx_rows)
        pair = (
            pairs[s * ctx_rows : (s + 1) * ctx_rows] * lax.rsqrt(mean + EPS) + ctx_add[:, att:]
        ).astype(bf16)
        CK[own, :] = pair[:, :att]
        CV[own, pl.ds(0, att)] = pair[:, att:]

    loads[12].wait()

    def spread(side_):
        first = 0 if side_ == 0 else rows + HALO
        for r in range(HALO):
            pair = HR[side_, pl.ds(r * GRID_W, GRID_W), :].astype(f32)
            for b in range(BLOCKS):
                strip = pair[STARTS[b] : STARTS[b] + STRIP].astype(bf16)
                KS[b, first + r] = strip[:, :att]
                VS[b, first + r, :, pl.ds(0, LANES)] = strip[:, att:]

    def a_copy(c, slot):
        return pltpu.make_async_remote_copy(
            src_ref=AS.at[c],
            dst_ref=AR.at[tp if slot is None else c],
            send_sem=a_send.at[c],
            recv_sem=a_recv.at[tp if slot is None else c],
            device_id={"tp": c},
            device_id_type=MESH,
        )

    low = -(-HALO // crows)
    inner = n_tp - 2 * low
    outer = 2 * low

    def attend(k, carry):
        @pl.when(k == inner)
        def _():
            @pl.when(sp > 0)
            def _():
                h_copy(0).wait_recv()
                spread(0)

            @pl.when(sp < n_sp - 1)
            def _():
                h_copy(1).wait_recv()
                spread(1)

        e = lax.rem(tp + 1 + k, outer)
        c = jnp.where(
            k < inner, low + lax.rem(tp + k, inner), jnp.where(e < low, e, e + inner)
        )
        rv = jnp.where(
            (sp == 0) & (c < 2), c + 1, jnp.where((sp == n_sp - 1) & (c == n_tp - 1), 3, 0)
        )
        base = jnp.where(
            (rv == 1) | (rv == 2), HALO, jnp.where(rv == 3, rows + HALO - urows, c * crows)
        )
        qs = [QS[b, pl.ds(c * crows, crows)].reshape(qrows, LANES) for b in range(BLOCKS)]
        fars = dot_nt(jnp.concatenate(qs, axis=0), CK[...])
        near_exps, far_exps = [], []
        for b in range(BLOCKS):
            ks = KS[b, pl.ds(base, urows)].reshape(ukeys, LANES)
            table = TB[rv, VARIANT[b], :, :, :, pl.ds(0, ukeys)].reshape(qrows, ukeys)
            near = dot_nt(qs[b], ks) + table
            far = fars[b * qrows : (b + 1) * qrows]
            peak = jnp.maximum(
                jnp.max(near, axis=1, keepdims=True), jnp.max(far, axis=1, keepdims=True)
            )
            near_exps.append(jnp.exp(near - peak).astype(bf16))
            far_exps.append(jnp.exp(far - peak).astype(bf16))
        far_sums = dot(jnp.concatenate(far_exps, axis=0), CV[...])
        for b in range(BLOCKS):
            vs = VS[b, pl.ds(base, urows)].reshape(ukeys, 2 * LANES)
            both = dot(near_exps[b], vs) + far_sums[b * qrows : (b + 1) * qrows]
            value = (both[:, :LANES] / both[:, LANES:]).reshape(crows, 2, COL_BLOCK, LANES)
            for i in range(crows):
                AS[c, pl.ds(i * GRID_W + b * COL_BLOCK, COL_BLOCK), :] = jnp.where(
                    head0, value[i, 0], value[i, 1]
                ).astype(bf16)

        @pl.when(c != tp)
        def _():
            a_copy(c, None).start()

        return carry

    lax.fori_loop(0, n_tp, attend, 0)

    AR[tp] = AS[tp]

    def a_wait(k, c):
        a_copy(lax.rem(tp + k, n_tp), 1).wait_recv()
        return c

    lax.fori_loop(1, n_tp, a_wait, 0)
    merged = jnp.concatenate([AR[t] for t in range(n_tp)], axis=1)
    own = pl.ds(pl.multiple_of(tp * share, share), share)
    for t in range(n_tp):
        cols = pl.ds(t * ft, ft)
        branch = dot(merged, WO[:, cols])
        out[:, cols] = (X[own, cols].astype(f32) + R2[t, 2:3, :] * branch).astype(bf16)

    def p1_done(j, c):
        @pl.when(j != sp)
        def _():
            p1_copy(j, sp).wait_send()

        return c

    lax.fori_loop(0, LEADERS, p1_done, 0)

    def t_done(j, c):
        t_copy(j).wait_send()
        return c

    lax.fori_loop(begins, ends, t_done, 0)

    def c_done(j, c):
        @pl.when(j != sp)
        def _():
            c_copy(j, sp).wait_send()

        return c

    lax.fori_loop(0, n_sp, c_done, 0)

    def p2_done(k, c):
        p2_copy(k, None).wait_send()
        a_copy(lax.rem(tp + k, n_tp), None).wait_send()
        return c

    lax.fori_loop(1, n_tp, p2_done, 0)
    for piece in range(2):
        d_copy(piece, tp, 0).wait_send()
        for k in range(1, chips):
            x_copy(piece, far(k), tp).wait_send()
            d_copy(piece, far(k), k).wait_send()

    @pl.when(sp < n_sp - 1)
    def _():
        h_copy(0).wait_send()

    @pl.when(sp > 0)
    def _():
        h_copy(1).wait_send()


def local(n_sp, n_tp, *args):
    (
        latent,
        condition,
        context_tokens,
        context_condition,
        shift_weight,
        scale_weight,
        gate_weight,
        norm_gain,
        query_weight,
        key_weight,
        value_weight,
        out_weight,
        offset_bias,
    ) = args
    tokens, width = latent.shape
    inputs, ft = shift_weight.shape
    att = query_weight.shape[1]
    rows = tokens // GRID_W
    crows = rows // n_tp
    share = crows * GRID_W
    urows = crows + WIN_ROWS - 1
    ctx_rows = context_tokens.shape[0]
    table = -(-urows * STRIP // LANES) * LANES
    padded = rows + 2 * HALO
    operands = (
        latent,
        condition.reshape(n_sp, inputs),
        context_tokens,
        context_condition.reshape(n_sp, inputs),
        shift_weight,
        scale_weight,
        gate_weight,
        norm_gain.reshape(n_sp, inputs),
        query_weight,
        key_weight,
        value_weight,
        out_weight,
        jnp.transpose(offset_bias, (1, 0, 2)),
    )
    dma = pltpu.SemaphoreType.DMA
    scratch = [
        pltpu.VMEM((tokens, width), bf16),
        pltpu.VMEM((n_sp, inputs), bf16),
        pltpu.VMEM((n_sp, inputs), bf16),
        pltpu.VMEM((3, inputs, ft), bf16),
        pltpu.VMEM((n_sp, inputs), bf16),
        pltpu.VMEM((width, 3 * att), bf16),
        pltpu.VMEM((width, 3 * att), bf16),
        pltpu.VMEM(out_weight.shape, bf16),
        pltpu.VMEM((offset_bias.shape[1], 2, offset_bias.shape[2]), f32),
        pltpu.VMEM((2, 16, LANES), f32),
        pltpu.VMEM((3, 2, 2 * WIN_ROWS, COL_BLOCK, LANES), f32),
        pltpu.VMEM((4, 3, crows, 2, COL_BLOCK, table), f32),
        pltpu.VMEM((tokens, LANES), f32),
        pltpu.VMEM((8, ft), f32),
        pltpu.VMEM((n_sp, 8, ft), f32),
        pltpu.VMEM((8, ft), f32),
        pltpu.VMEM((n_tp, 8, ft), f32),
        pltpu.VMEM((32, width), bf16),
        pltpu.VMEM((width, 2 * att), bf16),
        pltpu.VMEM((n_sp, ctx_rows, width), bf16),
        pltpu.VMEM((n_sp * ctx_rows, att), bf16),
        pltpu.VMEM((n_sp * ctx_rows, 2 * LANES), bf16),
        pltpu.VMEM((BLOCKS, rows, 2, COL_BLOCK, LANES), bf16),
        pltpu.VMEM((BLOCKS, padded, STRIP, LANES), bf16),
        pltpu.VMEM((BLOCKS, padded, STRIP, 2 * LANES), bf16),
        pltpu.VMEM((2, HALO * GRID_W, 2 * att), bf16),
        pltpu.VMEM((2, HALO * GRID_W, 2 * att), bf16),
        pltpu.VMEM((n_tp, share, LANES), bf16),
        pltpu.VMEM((n_tp, share, LANES), bf16),
        dma((13,)),
        dma((n_sp,)),
        dma((n_sp,)),
        dma((n_tp,)),
        dma((n_tp,)),
        dma((n_sp,)),
        dma((n_sp,)),
        dma((2 * n_tp,)),
        dma((2 * n_tp,)),
        dma((2 * n_tp,)),
        dma((2 * n_tp,)),
        dma((n_sp,)),
        dma((1,)),
        pltpu.SemaphoreType.REGULAR((n_sp,)),
        dma((2,)),
        dma((2,)),
        dma((n_tp,)),
        dma((n_tp,)),
    ]
    operands = tuple(pltpu.with_memory_space_constraint(x, pltpu.HBM) for x in operands)
    return pl.pallas_call(
        functools.partial(kernel, n_sp, n_tp),
        out_shape=jax.ShapeDtypeStruct((share, width), bf16),
        in_specs=[pl.BlockSpec(memory_space=pl.ANY)] * len(operands),
        out_specs=pl.BlockSpec(memory_space=pltpu.VMEM),
        scratch_shapes=scratch,
        compiler_params=pltpu.CompilerParams(
            collective_id=0, has_side_effects=True, vmem_limit_bytes=46_000_000
        ),
    )(*operands)


def solution(mesh):
    placed = (
        P(("grp", "sp"), None),
        P("grp"),
        P(("grp", "sp"), None),
        P(),
        P("sp", "tp"),
        P("sp", "tp"),
        P("sp", "tp"),
        P(),
        P(None, "tp"),
        P(None, "tp"),
        P(None, "tp"),
        P(),
        P("tp", None, None),
    )
    return jax.shard_map(
        functools.partial(local, mesh.shape["sp"], mesh.shape["tp"]),
        mesh=mesh,
        in_specs=placed,
        out_specs=P(("grp", "sp", "tp"), None),
        check_vma=False,
    )
```
